32 devices in a mesh: sp: 8 (over z, core), tp: 4 (over y, x).
Axes of the slice: x: 2, y: 2, z: 4, core: 2. Of those that a mesh axis runs over, the one named last changes fastest.
Arguments:
- stream: bfloat16 [3072, 2048], P('sp'), may hold values from -6 to 6
- inner_act: bfloat16 [3072, 4096], P('sp', 'tp'), may hold values from -6 to 6
- gate_act: bfloat16 [3072, 4096], P('sp', 'tp'), may hold values from -6 to 6
- state_write: bfloat16 [3072, 16, 128], P('sp', 'tp'), may hold values from -6 to 6
- state_read: bfloat16 [3072, 16, 128], P('sp', 'tp'), may hold values from -6 to 6
- step_raw: bfloat16 [3072, 64], P('sp', 'tp'), may hold values from -4.6 to 4.1
- conv_inner: bfloat16 [4, 4096], P(None, 'tp'), may hold values from -3 to 3
- conv_write: bfloat16 [4, 16, 128], P(None, 'tp'), may hold values from -3 to 3
- conv_read: bfloat16 [4, 16, 128], P(None, 'tp'), may hold values from -3 to 3
- step_bias: float32 [64], P('tp'), may hold values from -0.5 to 0.5
- decay_log: float32 [64], P('tp'), may hold values from -13 to -2.52, as said below
- inner_gain: float32 [4096], P('tp'), may hold values from 0.1 to 1.9
- out_weight: bfloat16 [4096, 2048], P('tp'), may hold values from -0.09375 to 0.09375
- ffn_gain: float32 [2048], replicated, may hold values from 0.1 to 1.9
- expert_ids: int32 [3072, 2], P('sp'), may hold values from 0 to 31, all different within a row; in each aligned block of 384 rows (0 to 383, 384 to 767, ...) at most 48 rows name the same one
- expert_weights: float32 [3072, 2], P('sp'), may hold values from 0.1 to 1
- expert_gate: bfloat16 [32, 2048, 1024], P('sp', None, 'tp'), may hold values from -0.125 to 0.125
- expert_up: bfloat16 [32, 2048, 1024], P('sp', None, 'tp'), may hold values from -0.125 to 0.125
- expert_down: bfloat16 [32, 1024, 2048], P('sp', None, 'tp'), may hold values from -0.1875 to 0.1875
Outputs:
- layer_out: bfloat16 [3072, 2048], P('sp', 'tp')
The draws below stay inside these ranges and needn't reach their ends.
Inputs may be any that keep to these rules, and one draw needn't show every extreme that they name: The logarithm of a per-position decay rate: exp(decay_log) lies between 0.1 / 3072 and 0.08. `expert_ids`: each row names 2 different experts. Among the rows of one index of sp (384 tokens) no expert is named more than 48 times, a bound that some block reaches there.
All inputs are finite; a program needn't handle non-finite values.
Results may differ from the reference program's by a relative error of at most 0.014.
Values may be sent and summed in bfloat16 or wider, within the bound.
No kernel may reach another device: no remote copies, remote signals or barrier semaphores. Data moves between devices by JAX's collectives and lax.ppermute only.
A program may use at most 64 MiB of HBM per device.

```python
import math
import jax
import jax.numpy as jnp
import numpy as np
from jax import lax

D = 2048
HEADS = 64
HEADDIM = 64
GROUPS = 16
STATE = 128
CONV = 4
BLOCK = 64
FF = 1024
EXPERTS = 32
TOPK = 2
TOK_SP = 384
D_INNER = 4096
TOKENS = 3072
CAP = 48
N_SP = 8
N_TP = 4


def draw_step_raw(key, part):
    key_noise, key_device, key_block = jax.random.split(jax.random.fold_in(key, 11), 3)
    jitter = 0.7 * jax.random.truncated_normal(key_noise, -3.0, 3.0, (TOKENS, HEADS), jnp.float32)
    device_shift = jax.random.uniform(key_device, (TOKENS // TOK_SP, 1, HEADS), jnp.float32, -2.0, 1.5)
    block_shift = jax.random.uniform(key_block, (TOKENS // BLOCK, 1, HEADS), jnp.float32, -0.5, 0.5)
    shifted = jitter.reshape(TOKENS // TOK_SP, TOK_SP, HEADS) + device_shift
    shifted = shifted.reshape(TOKENS // BLOCK, BLOCK, HEADS) + block_shift
    return shifted.reshape(TOKENS, HEADS).astype(jnp.bfloat16)


def draw_decay_log(key, part):
    key_pick, key_level = jax.random.split(jax.random.fold_in(key, 23))
    slow_share = 0.5
    slower = jax.random.bernoulli(key_pick, slow_share, (HEADS,))
    level = jax.random.uniform(key_level, (HEADS,), jnp.float32)
    slow_log = math.log(0.1) + level * math.log(5.0) - math.log(TOKENS)
    fast_log = math.log(0.02) + level * math.log(4.0)
    return jnp.where(slower, slow_log, fast_log).astype(jnp.float32)


def level_of(key, extent, cuts, smallest, high):
    gain, own = 1.0, jax.random.fold_in(key, 6)
    for dim, shards_of in cuts:
        steps = jnp.exp(jax.random.uniform(jax.random.fold_in(own, dim), (shards_of,), jnp.float32, smallest / len(cuts), high / len(cuts)))
        gain = gain * jnp.repeat(steps, extent[dim] // shards_of).reshape([-1 if axis == dim else 1 for axis in range(len(extent))])
    return gain


def routed_block(rng, own, number, rows, count, top, bound, skew):
    order = jax.random.permutation(rng, count)
    packed, ordinary = shares(count, rows * top, bound, skew, True), shares(count, rows * top, bound, skew, False)
    places = jnp.arange(count)

    def named(tallies, rotation):
        used = int((tallies > 0).sum())
        fixed = max(1, used // 4)
        passed = fixed + (places - fixed + rotation * (used - fixed)) % max(1, count - fixed)
        return jnp.zeros((count,), jnp.int32).at[order[jnp.where(places < fixed, places, passed)]].set(jnp.asarray(tallies, jnp.int32))

    tallies = jnp.where(number % 4 == 0, named(packed, number // 4), named(ordinary, number - number // 4 - 1))
    mixed = jax.random.permutation(jax.random.fold_in(own, 3), count)
    donor, receiver = mixed[0:count // 2 * 2:2], mixed[1:count // 2 * 2:2]
    room = jnp.minimum(tallies[donor] - 1, bound - tallies[receiver]) // 2
    room = jnp.where((donor == order[0]) | (receiver == order[0]) | (tallies[receiver] == 0), 0, jnp.maximum(room, 0))
    passed = jax.random.randint(jax.random.fold_in(own, 4), (count // 2,), 0, 1 << 20) % (room + 1)
    tallies = tallies.at[donor].add(-passed).at[receiver].add(passed)
    members = jnp.searchsorted(jnp.cumsum(tallies), jnp.arange(rows * top), side="right").astype(jnp.int32)
    listing = members.reshape(top, rows).T
    listing = listing[jax.random.permutation(jax.random.fold_in(own, 1), rows)]
    rotation = jax.random.randint(jax.random.fold_in(own, 2), (rows, 1), 0, top)
    return jnp.take_along_axis(listing, (jnp.arange(top)[None, :] + rotation) % top, axis=1)


def shares(count, total, bound, slope, full):
    weights = [(1 << 20) // math.isqrt(standing ** slope) + 1 for standing in range(1, count + 1)]
    largest = bound if full else min(bound, max(-(-total // count), total * weights[0] // sum(weights)))
    least = 1 if total - largest >= count - 1 else 0
    holding, rest = [largest] + [least] * (count - 1), total - largest - least * (count - 1)
    while rest > 0:
        candidates = [i for i in range(1, count) if holding[i] < largest] or [i for i in range(1, count) if holding[i] < bound]
        whole, budget = sum([weights[i] for i in candidates]), rest
        for i in candidates:
            extra = min(bound - holding[i], max(1, budget * weights[i] // whole), rest)
            holding[i] = holding[i] + extra
            rest = rest - extra
    return np.array(holding)


def centred(stream_key, shape, scale, limit, shards=(), held_as=jnp.bfloat16):
    loudness = level_of(stream_key, shape, shards, -0.22, 0.18) if shards else 1.0
    result = jax.random.normal(stream_key, shape, jnp.float32) * scale * loudness
    return jnp.minimum(jnp.maximum(result, -limit), limit).astype(held_as)


def setup_inputs(seed: int = 0) -> dict:
    seeds = jax.random.split(jax.random.key(seed), 20)
    stream = centred(seeds[0], (TOKENS, D), 1.0, 6.0, ((0, 8),))
    inner_act = centred(seeds[1], (TOKENS, D_INNER), 1.0, 6.0, ((0, 8), (1, 4)))
    gate_act = centred(seeds[2], (TOKENS, D_INNER), 1.0, 6.0, ((0, 8), (1, 4)))
    state_write = centred(seeds[3], (TOKENS, GROUPS, STATE), 1.0, 6.0, ((0, 8), (1, 4)))
    state_read = centred(seeds[4], (TOKENS, GROUPS, STATE), 1.0, 6.0, ((0, 8), (1, 4)))
    step_raw = draw_step_raw(jax.random.fold_in(seeds[19], 71), 0)
    conv_inner = centred(seeds[6], (CONV, D_INNER), 0.5, 3.0, ((1, 4),))
    conv_write = centred(seeds[7], (CONV, GROUPS, STATE), 0.5, 3.0, ((1, 4),))
    conv_read = centred(seeds[8], (CONV, GROUPS, STATE), 0.5, 3.0, ((1, 4),))
    step_bias = jnp.clip(jax.random.uniform(seeds[9], (HEADS,), jnp.float32, -0.5, 0.5) * level_of(seeds[9], (HEADS,), ((0, 4),), -0.4, 0.0), -0.5, 0.5)
    decay_log = draw_decay_log(jax.random.fold_in(seeds[19], 71), 0)
    inner_gain = jnp.clip(1.0 + 0.18 * jax.random.normal(seeds[11], (D_INNER,), jnp.float32), 0.1, 1.9)
    out_weight = centred(seeds[12], (D_INNER, D), D_INNER ** -0.5, 0.09375, ((0, 4),))
    ffn_gain = jnp.clip(1.0 + 0.18 * jax.random.normal(seeds[13], (D,), jnp.float32), 0.1, 1.9)
    expert_ids_keys = jax.random.split(jax.random.fold_in(seeds[14], 1), TOKENS // TOK_SP)
    expert_ids_turns = jax.random.permutation(jax.random.fold_in(seeds[14], 3), TOKENS // TOK_SP)
    expert_ids = jax.vmap(lambda own, number: routed_block(jax.random.fold_in(seeds[14], 2), own, number, TOK_SP, EXPERTS, TOPK, CAP, 1))(expert_ids_keys, expert_ids_turns).reshape((TOKENS, TOPK))
    expert_weights = jnp.clip(0.1 + 0.9 * jax.random.uniform(seeds[15], (TOKENS, TOPK), jnp.float32) ** level_of(seeds[15], (TOKENS, TOPK), ((0, 8),), -0.2, 0.2), 0.1, 1.0)
    expert_gate = centred(seeds[16], (EXPERTS, D, FF), D ** -0.5, 0.125, ((0, 8), (2, 4)))
    expert_up = centred(seeds[17], (EXPERTS, D, FF), D ** -0.5, 0.125, ((0, 8), (2, 4)))
    expert_down = centred(seeds[18], (EXPERTS, FF, D), FF ** -0.5, 0.1875, ((0, 8), (2, 4)))
    return {"stream": stream, "inner_act": inner_act, "gate_act": gate_act, "state_write": state_write, "state_read": state_read, "step_raw": step_raw, "conv_inner": conv_inner, "conv_write": conv_write, "conv_read": conv_read, "step_bias": step_bias, "decay_log": decay_log, "inner_gain": inner_gain, "out_weight": out_weight, "ffn_gain": ffn_gain, "expert_ids": expert_ids, "expert_weights": expert_weights, "expert_gate": expert_gate, "expert_up": expert_up, "expert_down": expert_down}


HIGH = lax.Precision.HIGHEST
EPS = 1e-06

def conv_silu(padded, weights, length):
    running = jnp.zeros((length, padded.shape[1]), jnp.float32)
    for offset in range(weights.shape[0]):
        running = running + weights[offset][None, :] * padded[offset:offset + length]
    return jax.nn.silu(running)

def block_terms(values, step_len, decay_rate, writes, reads, block_len):
    blocks = values.shape[0] // block_len
    groups, per_group, head_dim = (values.shape[1], values.shape[2], values.shape[3])
    state_dim = writes.shape[2]
    value_blk = values.reshape(blocks, block_len, groups, per_group, head_dim)
    step_blk = step_len.reshape(blocks, block_len, groups, per_group)
    write_blk = writes.reshape(blocks, block_len, groups, state_dim)
    read_blk = reads.reshape(blocks, block_len, groups, state_dim)
    cumul = jnp.cumsum(step_blk * decay_rate, axis=1)
    causal = jnp.tril(jnp.ones((block_len, block_len), dtype=bool))[None, :, :, None, None]
    spread = cumul[:, :, None] - cumul[:, None, :]
    within = jnp.where(causal, jnp.exp(jnp.where(causal, spread, 0.0)), 0.0)
    intersect = jnp.einsum('clgn,csgn->clsg', read_blk, write_blk, precision=HIGH)
    mixing = intersect[..., None] * within * step_blk[:, None]
    inside = jnp.einsum('clsgh,csghp->clghp', mixing, value_blk, precision=HIGH)
    to_end = jnp.exp(cumul[:, -1:] - cumul) * step_blk
    block_state = jnp.einsum('clgn,clghp->cghpn', write_blk, to_end[..., None] * value_blk, precision=HIGH)
    block_decay = jnp.exp(cumul[:, -1])

    def advance(carried, inputs):
        state_here, decay_here = inputs
        return (carried * decay_here[..., None, None] + state_here, carried)
    initial = jnp.zeros(block_state.shape[1:], jnp.float32)
    closing, entering = lax.scan(advance, initial, (block_state, block_decay))
    return (inside, entering, cumul, read_blk, closing)

def convolve(source, kernel):
    channels = source.shape[1]
    padded = jnp.concatenate([jnp.zeros((CONV - 1, channels), jnp.float32), source.astype(jnp.float32)], axis=0)
    return conv_silu(padded, kernel.astype(jnp.float32).reshape(CONV, channels), TOKENS)

def reference(stream, inner_act, gate_act, state_write, state_read, step_raw, conv_inner, conv_write, conv_read, step_bias, decay_log, inner_gain, out_weight, ffn_gain, expert_ids, expert_weights, expert_gate, expert_up, expert_down):
    per_group = HEADS // GROUPS
    write_width = GROUPS * STATE
    values = convolve(inner_act, conv_inner).reshape(TOKENS, GROUPS, per_group, HEADDIM)
    writes = convolve(state_write.reshape(TOKENS, write_width), conv_write).reshape(TOKENS, GROUPS, STATE)
    reads = convolve(state_read.reshape(TOKENS, write_width), conv_read).reshape(TOKENS, GROUPS, STATE)
    step_len = jax.nn.softplus(step_raw.astype(jnp.float32) + step_bias[None, :]).reshape(TOKENS, GROUPS, per_group)
    decay_rate = (-jnp.exp(decay_log)).reshape(GROUPS, per_group)
    inside, entering, cumul, read_blk, closing = block_terms(values, step_len, decay_rate, writes, reads, BLOCK)
    outside = jnp.einsum('clgn,cghpn->clghp', read_blk, entering, precision=HIGH) * jnp.exp(cumul)[..., None]
    gated = (inside + outside).reshape(TOKENS, D_INNER) * jax.nn.silu(gate_act.astype(jnp.float32))
    per_head = gated.reshape(TOKENS, HEADS, HEADDIM)
    per_head = per_head * lax.rsqrt(lax.optimization_barrier(jnp.mean(per_head * per_head, axis=-1, keepdims=True)) + EPS)
    mixed_inner = (per_head.reshape(TOKENS, D_INNER) * inner_gain[None, :]).astype(jnp.bfloat16)
    block_width = D_INNER // N_TP

    def add_block(index, running):
        begin = (index * block_width).astype(jnp.int32)
        columns = lax.dynamic_slice_in_dim(mixed_inner, begin, block_width, 1)
        weight_rows = lax.dynamic_slice_in_dim(out_weight, begin, block_width, 0)
        partial_value = jnp.dot(columns, weight_rows, preferred_element_type=jnp.float32).astype(jnp.bfloat16)
        partial_value = lax.optimization_barrier(partial_value)
        return running + partial_value.astype(jnp.float32)
    projected = lax.fori_loop(0, N_TP, add_block, jnp.zeros((TOKENS, D), jnp.float32))
    middle = stream.astype(jnp.float32) + projected
    normed = (middle * lax.rsqrt(lax.optimization_barrier(jnp.mean(middle * middle, axis=-1, keepdims=True)) + EPS) * ffn_gain[None, :]).astype(jnp.bfloat16)
    per_block = TOK_SP * TOPK
    choices_blk = expert_ids.reshape(N_SP, per_block)
    onehot = (choices_blk[..., None] == jnp.arange(EXPERTS, dtype=jnp.int32)[None, None, :]).astype(jnp.int32)
    earlier_count = jnp.cumsum(onehot, axis=1) - onehot
    slot_of = lax.optimization_barrier(jnp.sum(earlier_count * onehot, axis=-1))
    owner = jnp.arange(N_SP, dtype=jnp.int32)[:, None]
    target = (choices_blk * (N_SP * CAP) + owner * CAP + slot_of).reshape(-1).astype(jnp.int32)
    token_of = (jnp.arange(TOKENS * TOPK, dtype=jnp.int32) // TOPK).astype(jnp.int32)
    slot_table = jnp.full((EXPERTS * N_SP * CAP,), TOKENS, jnp.int32).at[target].set(token_of)
    slot_table = slot_table.reshape(EXPERTS, N_SP * CAP)
    padded_rows = jnp.concatenate([normed, jnp.zeros((1, D), jnp.bfloat16)], axis=0)

    def one_expert(index):
        tok_rows = padded_rows[slot_table[index]]
        gate_part = jnp.dot(tok_rows, expert_gate[index], preferred_element_type=jnp.float32)
        up_part = jnp.dot(tok_rows, expert_up[index], preferred_element_type=jnp.float32)
        hidden = (jax.nn.silu(gate_part) * up_part).astype(jnp.bfloat16)
        return jnp.dot(hidden, expert_down[index], preferred_element_type=jnp.float32).astype(jnp.bfloat16)
    results = lax.map(one_expert, jnp.arange(EXPERTS, dtype=jnp.int32))
    results = results.reshape(EXPERTS * N_SP * CAP, D)
    picked = results[target].astype(jnp.float32).reshape(TOKENS, TOPK, D)
    moe = lax.optimization_barrier(jnp.sum(picked * expert_weights[:, :, None], axis=1))
    return (middle + moe).astype(jnp.bfloat16)
```

```python
import jax
import jax.numpy as jnp
from jax import lax
from jax.experimental import pallas as pl
from jax.experimental.pallas import tpu as pltpu
from jax.sharding import PartitionSpec as P

BLOCK = 64
TOPK = 2
CAP = 48


HIGH = lax.Precision.HIGHEST
EPS = 1e-06


def from_behind(value, axis, steps):
    count = lax.axis_size(axis)
    first, last = (max(0, -steps), min(count, count - steps))
    return lax.ppermute(value, axis, [(source, source + steps) for source in range(first, last)])


def carried_in(value, axis, join, neutral):
    place = lax.axis_index(axis)
    gathered = jax.tree.map(
        lambda a, kind: lax.all_gather(a.astype(kind), axis), value, (jnp.bfloat16, jnp.bfloat16)
    )
    state = jax.tree.map(lambda a, e: jnp.zeros_like(a) + jnp.asarray(e, a.dtype), value, neutral)

    def one(turn, state):
        return join(
            state,
            jax.tree.map(
                lambda a, own: lax.dynamic_index_in_dim(a, turn, 0, False).astype(own.dtype),
                gathered,
                value,
            ),
        )

    return lax.fori_loop(0, place, one, state)


def swap_core(value):
    count = lax.axis_size("sp")
    return lax.ppermute(value, "sp", [(i, i ^ 1) for i in range(count)])


def move_chips(value, steps, cross=False):
    count = lax.axis_size("sp")
    return lax.ppermute(
        value, "sp", [(i, ((i + 2 * steps) % count) ^ int(cross)) for i in range(count)]
    )


def swap_tp(value, mask):
    count = lax.axis_size("tp")
    return lax.ppermute(value, "tp", [(i, i ^ mask) for i in range(count)])


def gather_tp(rows):
    count = lax.axis_size("tp")
    if count != 4:
        every = lax.all_gather(rows, "tp")
        own = lax.axis_index("tp")
        return [lax.dynamic_index_in_dim(every, own ^ m, 0, False) for m in range(count)]
    half = rows.shape[0] // 2
    from_x = swap_tp(rows, 1)
    from_y = swap_tp(rows, 2)
    first = swap_tp(from_x[:half], 2)
    second = swap_tp(from_y[half:], 1)
    return [rows, from_x, from_y, jnp.concatenate([first, second], axis=0)]


def sum_tp(value):
    count = lax.axis_size("tp")
    parts = [swap_tp(value, m) for m in range(1, count)]
    for part in parts:
        value = value + part
    return value


def ranks_of(ids, first, count):
    tokens = ids.shape[1]
    experts = first + jnp.arange(count, dtype=jnp.int32)
    named = (ids[0][None, :] == experts[:, None]) | (ids[1][None, :] == experts[:, None])
    earlier = jnp.arange(tokens)[:, None] < jnp.arange(tokens)[None, :]
    slots = jnp.dot(
        named.astype(jnp.bfloat16),
        earlier.astype(jnp.bfloat16),
        preferred_element_type=jnp.float32,
    )
    return jnp.where(named, slots.astype(jnp.int32), -1)


def pick_rows(same, other, rank_same, rank_other):
    experts = rank_same.shape[0]
    tokens, width = same.shape

    def kernel(same_ref, other_ref, rank_same_ref, rank_other_ref, out_ref):
        slot = lax.broadcasted_iota(jnp.int32, (CAP, tokens), 0)
        for side, (rows, rank) in enumerate(
            ((same_ref, rank_same_ref), (other_ref, rank_other_ref))
        ):
            chosen = jnp.concatenate(
                [(rank[e : e + 1, :] == slot).astype(jnp.float32) for e in range(experts)], axis=0
            ).astype(jnp.bfloat16)
            picked = jnp.dot(chosen, rows[...], preferred_element_type=jnp.float32)
            picked = picked.astype(jnp.bfloat16)
            for e in range(experts):
                out_ref[e, side] = picked[e * CAP : (e + 1) * CAP]

    return pl.pallas_call(
        kernel,
        out_shape=jax.ShapeDtypeStruct((experts, 2, CAP, width), jnp.bfloat16),
        cost_estimate=pl.CostEstimate(
            flops=4 * experts * CAP * tokens * width, bytes_accessed=8 * tokens * width, transcendentals=0
        ),
        name="pick_rows",
    )(same, other, rank_same, rank_other)


def hidden_units(pieces, gate, up, own):
    experts, full, units = gate.shape
    rows, width = pieces[0].shape
    each = rows // experts
    count = len(pieces)

    def kernel(own_ref, *refs):
        parts, (gate_ref, up_ref, out_ref) = refs[:count], refs[count:]
        gate_sum = jnp.zeros((each, units), jnp.float32)
        up_sum = jnp.zeros((each, units), jnp.float32)
        for m in range(count):
            start = pl.multiple_of((own_ref[0] ^ m) * width, width)
            part = parts[m][...]
            gate_sum += jnp.dot(
                part, gate_ref[0, pl.ds(start, width), :], preferred_element_type=jnp.float32
            )
            up_sum += jnp.dot(
                part, up_ref[0, pl.ds(start, width), :], preferred_element_type=jnp.float32
            )
        out_ref[...] = (gate_sum * jax.nn.sigmoid(gate_sum) * up_sum).astype(jnp.bfloat16)

    return pl.pallas_call(
        kernel,
        grid_spec=pltpu.PrefetchScalarGridSpec(
            num_scalar_prefetch=1,
            grid=(experts,),
            in_specs=[pl.BlockSpec((each, width), lambda e, o: (e, 0)) for _ in range(count)]
            + [pl.BlockSpec((1, full, units), lambda e, o: (e, 0, 0)) for _ in range(2)],
            out_specs=pl.BlockSpec((each, units), lambda e, o: (e, 0)),
        ),
        out_shape=jax.ShapeDtypeStruct((rows, units), jnp.bfloat16),
        cost_estimate=pl.CostEstimate(
            flops=4 * rows * full * units,
            bytes_accessed=4 * experts * full * units,
            transcendentals=rows * units,
        ),
        name="hidden_units",
    )(own, *pieces, gate, up)


def expert_rows(pieces, down, own):
    experts, full, columns = down.shape
    rows, units = pieces[0].shape
    each = rows // experts
    count = len(pieces)

    def kernel(own_ref, *refs):
        parts, (down_ref, out_ref) = refs[:count], refs[count:]
        total = jnp.zeros((each, columns), jnp.float32)
        for m in range(count):
            start = pl.multiple_of((own_ref[0] ^ m) * units, units)
            total += jnp.dot(
                parts[m][...], down_ref[0, pl.ds(start, units), :], preferred_element_type=jnp.float32
            )
        out_ref[0] = total[:CAP].astype(jnp.bfloat16)
        out_ref[1] = total[CAP:].astype(jnp.bfloat16)

    return pl.pallas_call(
        kernel,
        grid_spec=pltpu.PrefetchScalarGridSpec(
            num_scalar_prefetch=1,
            grid=(experts,),
            in_specs=[pl.BlockSpec((each, units), lambda e, o: (e, 0)) for _ in range(count)]
            + [pl.BlockSpec((1, full, columns), lambda e, o: (e, 0, 0))],
            out_specs=pl.BlockSpec((2, CAP, columns), lambda e, o: (0, e, 0)),
        ),
        out_shape=jax.ShapeDtypeStruct((2, experts * CAP, columns), jnp.bfloat16),
        cost_estimate=pl.CostEstimate(
            flops=2 * rows * full * columns,
            bytes_accessed=2 * experts * full * columns,
            transcendentals=0,
        ),
        name="expert_rows",
    )(own, *pieces, down)


def combine(kept, returned, ranks, shares):
    tokens, columns = kept.shape
    count = len(returned)
    experts = ranks[0].shape[0]

    def kernel(kept_ref, *refs):
        row_refs, rank_refs, share_refs = refs[:count], refs[count : 2 * count], refs[2 * count : -1]
        out_ref = refs[-1]
        slot = lax.broadcasted_iota(jnp.int32, (CAP, tokens), 0)
        total = kept_ref[...]
        for rows, rank, share in zip(row_refs, rank_refs, share_refs):
            chosen = jnp.concatenate(
                [
                    jnp.where(rank[e : e + 1, :] == slot, share[e : e + 1, :], 0.0)
                    for e in range(experts)
                ],
                axis=0,
            )
            high = chosen.astype(jnp.bfloat16)
            low = (chosen - high.astype(jnp.float32)).astype(jnp.bfloat16)
            for part in (high, low):
                total += lax.dot_general(
                    part, rows[...], (((0,), (0,)), ((), ())), preferred_element_type=jnp.float32
                )
        out_ref[...] = total.astype(jnp.bfloat16)

    return pl.pallas_call(
        kernel,
        out_shape=jax.ShapeDtypeStruct((tokens, columns), jnp.bfloat16),
        name="combine",
    )(kept, *returned, *ranks, *shares)


def conv_silu(padded, weights, length):
    running = jnp.zeros((length, padded.shape[1]), jnp.float32)
    for offset in range(weights.shape[0]):
        running = running + weights[offset][None, :] * padded[offset : offset + length]
    return jax.nn.silu(running)


def block_terms(values, step_len, decay_rate, writes, reads, block_len):
    blocks = values.shape[0] // block_len
    groups, per_group, head_dim = (values.shape[1], values.shape[2], values.shape[3])
    state_dim = writes.shape[2]
    value_blk = values.reshape(blocks, block_len, groups, per_group, head_dim)
    step_blk = step_len.reshape(blocks, block_len, groups, per_group)
    write_blk = writes.reshape(blocks, block_len, groups, state_dim)
    read_blk = reads.reshape(blocks, block_len, groups, state_dim)
    cumul = jnp.cumsum(step_blk * decay_rate, axis=1)
    causal = jnp.tril(jnp.ones((block_len, block_len), dtype=bool))[None, :, :, None, None]
    spread = cumul[:, :, None] - cumul[:, None, :]
    within = jnp.where(causal, jnp.exp(jnp.where(causal, spread, 0.0)), 0.0)
    intersect = jnp.einsum("clgn,csgn->clsg", read_blk, write_blk, precision=HIGH)
    mixing = intersect[..., None] * within * step_blk[:, None]
    inside = jnp.einsum("clsgh,csghp->clghp", mixing, value_blk, precision=HIGH)
    to_end = jnp.exp(cumul[:, -1:] - cumul) * step_blk
    block_state = jnp.einsum(
        "clgn,clghp->cghpn", write_blk, to_end[..., None] * value_blk, precision=HIGH
    )
    block_decay = jnp.exp(cumul[:, -1])

    def advance(carried, inputs):
        state_here, decay_here = inputs
        return (carried * decay_here[..., None, None] + state_here, carried)

    initial = jnp.zeros(block_state.shape[1:], jnp.float32)
    closing, entering = lax.scan(advance, initial, (block_state, block_decay))
    return (inside, entering, cumul, read_blk, closing)


def chain(earlier_part, later_part):
    return (
        earlier_part[0] * later_part[0],
        earlier_part[1] * later_part[0][..., None, None] + later_part[1],
    )


def per_device(
    stream,
    inner_act,
    gate_act,
    state_write,
    state_read,
    step_raw,
    conv_inner,
    conv_write,
    conv_read,
    step_bias,
    decay_log,
    inner_gain,
    out_weight,
    ffn_gain,
    expert_ids,
    expert_weights,
    expert_gate,
    expert_up,
    expert_down,
):
    length = inner_act.shape[0]
    heads_here = step_raw.shape[1]
    groups_here = state_write.shape[1]
    state_dim = state_write.shape[2]
    inner_width = inner_act.shape[1]
    head_dim = inner_width // heads_here
    per_group = heads_here // groups_here
    write_width = groups_here * state_dim
    joined = jnp.concatenate(
        [
            inner_act,
            state_write.reshape(length, write_width),
            state_read.reshape(length, write_width),
        ],
        axis=1,
    )
    kernel = jnp.concatenate(
        [conv_inner, conv_write.reshape(-1, write_width), conv_read.reshape(-1, write_width)],
        axis=1,
    ).astype(jnp.float32)
    lag_rows = kernel.shape[0] - 1
    earlier = from_behind(joined[length - lag_rows :], "sp", 1)
    padded = jnp.concatenate([earlier, joined], axis=0).astype(jnp.float32)
    conv_out = conv_silu(padded, kernel, length)
    values = conv_out[:, :inner_width].reshape(length, groups_here, per_group, head_dim)
    writes = conv_out[:, inner_width : inner_width + write_width].reshape(
        length, groups_here, state_dim
    )
    reads = conv_out[:, inner_width + write_width :].reshape(length, groups_here, state_dim)
    step_len = jax.nn.softplus(step_raw.astype(jnp.float32) + step_bias[None, :]).reshape(
        length, groups_here, per_group
    )
    decay_rate = (-jnp.exp(decay_log)).reshape(groups_here, per_group)
    inside, entering, cumul, read_blk, closing = block_terms(
        values, step_len, decay_rate, writes, reads, BLOCK
    )
    block_sums = cumul[:, -1]
    device_decay = jnp.exp(jnp.sum(block_sums, axis=0))
    unused_decay, arriving = carried_in(
        (device_decay, closing), "sp", chain, (jnp.ones_like(device_decay), jnp.zeros_like(closing))
    )
    before = jnp.exp(jnp.cumsum(block_sums, axis=0) - block_sums)
    entering = entering + arriving[None] * before[..., None, None]
    outside = (
        jnp.einsum("clgn,cghpn->clghp", read_blk, entering, precision=HIGH)
        * jnp.exp(cumul)[..., None]
    )
    gated = (inside + outside).reshape(length, inner_width) * jax.nn.silu(
        gate_act.astype(jnp.float32)
    )
    per_head = gated.reshape(length, heads_here, head_dim)
    per_head = per_head * lax.rsqrt(jnp.mean(per_head * per_head, axis=-1, keepdims=True) + EPS)
    mixed_inner = (per_head.reshape(length, inner_width) * inner_gain[None, :]).astype(jnp.bfloat16)
    partial_value = jnp.dot(mixed_inner, out_weight, preferred_element_type=jnp.float32)
    full_width = partial_value.shape[1]
    local_experts = expert_gate.shape[0]
    out_width = expert_down.shape[2]
    tp_count = lax.axis_size("tp")
    chips = lax.axis_size("sp") // 2
    own_tp = lax.axis_index("tp")
    own_sp = lax.axis_index("sp")
    own_start = own_tp * out_width
    ids_own = expert_ids.T
    ids_pair = jnp.stack([ids_own, swap_core(ids_own)])
    ids_of = [ids_pair] + [move_chips(ids_pair, k) for k in range(1, chips)]
    arriving_ranks = [
        [ranks_of(ids_of[k][side], own_sp * local_experts, local_experts) for side in range(2)]
        for k in range(chips)
    ]
    weights_own = expert_weights.T
    leaving_ranks, leaving_shares = [], []
    for k in range(chips):
        for side in range(2):
            owner = ((own_sp + 2 * k) % (2 * chips)) ^ side
            first = owner * local_experts
            leaving_ranks.append(ranks_of(ids_own, first, local_experts))
            experts = first + jnp.arange(local_experts, dtype=jnp.int32)
            leaving_shares.append(
                sum(
                    jnp.where(ids_own[j][None, :] == experts[:, None], weights_own[j][None, :], 0.0)
                    for j in range(TOPK)
                )
            )
    partial_value = partial_value.astype(jnp.bfloat16)
    projected = lax.dynamic_slice_in_dim(partial_value, own_start, out_width, 1).astype(jnp.float32)
    leaving = [
        lax.dynamic_slice_in_dim(partial_value, (own_tp ^ m) * out_width, out_width, 1)
        for m in range(1, tp_count)
    ]
    for part in [swap_tp(leaving[m - 1], m) for m in reversed(range(1, tp_count))]:
        projected = projected + part.astype(jnp.float32)
    kept = lax.dynamic_slice_in_dim(stream, own_start, out_width, 1).astype(jnp.float32) + projected
    square_total = sum_tp(jnp.sum(kept * kept, axis=1))
    gain_share = lax.dynamic_slice_in_dim(ffn_gain, own_start, out_width, 0)
    scale_rows = lax.rsqrt(square_total / full_width + EPS)
    normed = (kept * scale_rows[:, None] * gain_share[None, :]).astype(jnp.bfloat16)
    own_index = own_tp.astype(jnp.int32).reshape(1)
    returned = []
    current = normed
    for k in range(chips):
        if k:
            current = move_chips(current, 1)
        picked = pick_rows(current, swap_core(current), *arriving_ranks[k])
        picked = picked.reshape(-1, out_width)
        hidden = hidden_units(gather_tp(picked), expert_gate, expert_up, own_index)
        given = expert_rows(gather_tp(hidden), expert_down, own_index)
        returned.append(move_chips(given[0], -k) if k else given[0])
        returned.append(move_chips(given[1], -k, True))
    return combine(kept, returned, leaving_ranks, leaving_shares)


def solution(mesh):
    return jax.shard_map(
        per_device,
        mesh=mesh,
        in_specs=(
            P("sp", None),
            P("sp", "tp"),
            P("sp", "tp"),
            P("sp", "tp", None),
            P("sp", "tp", None),
            P("sp", "tp"),
            P(None, "tp"),
            P(None, "tp", None),
            P(None, "tp", None),
            P("tp"),
            P("tp"),
            P("tp"),
            P("tp", None),
            P(),
            P("sp", None),
            P("sp", None),
            P("sp", None, "tp"),
            P("sp", None, "tp"),
            P("sp", None, "tp"),
        ),
        out_specs=P("sp", "tp"),
        check_vma=False,
    )
```

```python
import jax
import jax.numpy as jnp
from jax import lax
from jax.experimental import pallas as pl
from jax.experimental.pallas import tpu as pltpu
from jax.sharding import PartitionSpec as P

SPAN = 128
LEAD = 16
CHUNK = 2
TOPK = 2
CAP = 48


EPS = 1e-06


def from_behind(value, axis, steps):
    count = lax.axis_size(axis)
    first, last = (max(0, -steps), min(count, count - steps))
    return lax.ppermute(value, axis, [(source, source + steps) for source in range(first, last)])


def silu(x):
    return x * (0.5 * jnp.tanh(0.5 * x) + 0.5)


def swap_core(value):
    count = lax.axis_size("sp")
    return lax.ppermute(value, "sp", [(i, i ^ 1) for i in range(count)])


def move_chips(value, steps, cross=False):
    count = lax.axis_size("sp")
    return lax.ppermute(
        value, "sp", [(i, ((i + 2 * steps) % count) ^ int(cross)) for i in range(count)]
    )


def swap_tp(value, mask):
    count = lax.axis_size("tp")
    return lax.ppermute(value, "tp", [(i, i ^ mask) for i in range(count)])


def gather_tp(rows):
    count = lax.axis_size("tp")
    if count != 4:
        every = lax.all_gather(rows, "tp")
        own = lax.axis_index("tp")
        return [lax.dynamic_index_in_dim(every, own ^ m, 0, False) for m in range(count)]
    half = rows.shape[0] // 2
    from_x = swap_tp(rows, 1)
    from_y = swap_tp(rows, 2)
    first = swap_tp(from_x[:half], 2)
    second = swap_tp(from_y[half:], 1)
    return [rows, from_x, from_y, first, second]


def piece_specs(pieces, experts, each, width):
    rows = pieces[0].shape[0]
    half = experts // 2
    specs = []
    for piece in pieces:
        if piece.shape[0] == rows:
            specs.append(pl.BlockSpec((each, width), lambda e, o: (e, 0)))
        elif len(specs) == len(pieces) - 2:
            specs.append(pl.BlockSpec((each, width), lambda e, o: (jnp.minimum(e, half - 1), 0)))
        else:
            specs.append(pl.BlockSpec((each, width), lambda e, o: (jnp.maximum(e - half, 0), 0)))
    return specs


def read_pieces(refs, experts, halved):
    if not halved:
        return [ref[...] for ref in refs]
    early = pl.program_id(0) < experts // 2
    return [ref[...] for ref in refs[:-2]] + [jnp.where(early, refs[-2][...], refs[-1][...])]


def sum_tp(value):
    count = lax.axis_size("tp")
    parts = [swap_tp(value, m) for m in range(1, count)]
    for part in parts:
        value = value + part
    return value


def ranks_of(ids, first, count):
    tokens = ids.shape[1]
    experts = first + jnp.arange(count, dtype=jnp.int32)
    named = (ids[0][None, :] == experts[:, None]) | (ids[1][None, :] == experts[:, None])
    earlier = jnp.arange(tokens)[:, None] < jnp.arange(tokens)[None, :]
    slots = jnp.dot(
        named.astype(jnp.bfloat16),
        earlier.astype(jnp.bfloat16),
        preferred_element_type=jnp.float32,
    )
    return jnp.where(named, slots.astype(jnp.int32), -1)


def pick_rows(blocks, ranks):
    experts = ranks[0].shape[0]
    tokens, width = blocks[0].shape
    count = len(blocks)

    def kernel(*refs):
        block_refs, rank_refs, out_ref = refs[:count], refs[count:-1], refs[-1]
        slot = lax.broadcasted_iota(jnp.int32, (CAP, tokens), 0)
        for side, (rows, rank) in enumerate(zip(block_refs, rank_refs)):
            chosen = jnp.concatenate(
                [(rank[e : e + 1, :] == slot).astype(jnp.float32) for e in range(experts)], axis=0
            ).astype(jnp.bfloat16)
            picked = jnp.dot(chosen, rows[...], preferred_element_type=jnp.float32)
            picked = picked.astype(jnp.bfloat16)
            for e in range(experts):
                out_ref[e, side] = picked[e * CAP : (e + 1) * CAP]

    return pl.pallas_call(
        kernel,
        out_shape=jax.ShapeDtypeStruct((experts, count, CAP, width), jnp.bfloat16),
        cost_estimate=pl.CostEstimate(
            flops=2 * count * experts * CAP * tokens * width,
            bytes_accessed=4 * count * tokens * width,
            transcendentals=0,
        ),
        name="pick_rows",
    )(*blocks, *ranks)


def hidden_units(pieces, gate, up, own):
    experts, full, units = gate.shape
    rows, width = pieces[0].shape
    each = rows // experts
    count = len(pieces)
    halved = pieces[-1].shape[0] != rows

    def kernel(own_ref, *refs):
        parts, (gate_ref, up_ref, out_ref) = refs[:count], refs[count:]
        gate_sum = jnp.zeros((each, units), jnp.float32)
        up_sum = jnp.zeros((each, units), jnp.float32)
        for m, part in enumerate(read_pieces(parts, experts, halved)):
            start = pl.multiple_of((own_ref[0] ^ m) * width, width)
            gate_sum += jnp.dot(
                part, gate_ref[0, pl.ds(start, width), :], preferred_element_type=jnp.float32
            )
            up_sum += jnp.dot(
                part, up_ref[0, pl.ds(start, width), :], preferred_element_type=jnp.float32
            )
        out_ref[...] = (silu(gate_sum) * up_sum).astype(jnp.bfloat16)

    return pl.pallas_call(
        kernel,
        grid_spec=pltpu.PrefetchScalarGridSpec(
            num_scalar_prefetch=1,
            grid=(experts,),
            in_specs=piece_specs(pieces, experts, each, width)
            + [pl.BlockSpec((1, full, units), lambda e, o: (e, 0, 0)) for _ in range(2)],
            out_specs=pl.BlockSpec((each, units), lambda e, o: (e, 0)),
        ),
        out_shape=jax.ShapeDtypeStruct((rows, units), jnp.bfloat16),
        cost_estimate=pl.CostEstimate(
            flops=4 * rows * full * units,
            bytes_accessed=4 * experts * full * units,
            transcendentals=rows * units,
        ),
        name="hidden_units",
    )(own, *pieces, gate, up)


def expert_rows(pieces, down, own):
    experts, full, columns = down.shape
    rows, units = pieces[0].shape
    each = rows // experts
    blocks = each // CAP
    count = len(pieces)
    halved = pieces[-1].shape[0] != rows

    def kernel(own_ref, *refs):
        parts, (down_ref, out_ref) = refs[:count], refs[count:]
        total = jnp.zeros((each, columns), jnp.float32)
        for m, part in enumerate(read_pieces(parts, experts, halved)):
            start = pl.multiple_of((own_ref[0] ^ m) * units, units)
            total += jnp.dot(
                part, down_ref[0, pl.ds(start, units), :], preferred_element_type=jnp.float32
            )
        for i in range(blocks):
            out_ref[i] = total[i * CAP : (i + 1) * CAP].astype(jnp.bfloat16)

    return pl.pallas_call(
        kernel,
        grid_spec=pltpu.PrefetchScalarGridSpec(
            num_scalar_prefetch=1,
            grid=(experts,),
            in_specs=piece_specs(pieces, experts, each, units)
            + [pl.BlockSpec((1, full, columns), lambda e, o: (e, 0, 0))],
            out_specs=pl.BlockSpec((blocks, CAP, columns), lambda e, o: (0, e, 0)),
        ),
        out_shape=jax.ShapeDtypeStruct((blocks, experts * CAP, columns), jnp.bfloat16),
        cost_estimate=pl.CostEstimate(
            flops=2 * rows * full * columns,
            bytes_accessed=2 * experts * full * columns,
            transcendentals=0,
        ),
        name="expert_rows",
    )(own, *pieces, down)


def combine(kept, returned, ranks, shares):
    tokens, columns = kept.shape
    count = len(returned)
    experts = ranks[0].shape[0]

    def kernel(kept_ref, *refs):
        row_refs, rank_refs, share_refs = refs[:count], refs[count : 2 * count], refs[2 * count : -1]
        out_ref = refs[-1]
        slot = lax.broadcasted_iota(jnp.int32, (CAP, tokens), 0)
        total = kept_ref[...]
        for rows, rank, share in zip(row_refs, rank_refs, share_refs):
            chosen = jnp.concatenate(
                [
                    jnp.where(rank[e : e + 1, :] == slot, share[e : e + 1, :], 0.0)
                    for e in range(experts)
                ],
                axis=0,
            )
            high = chosen.astype(jnp.bfloat16)
            low = (chosen - high.astype(jnp.float32)).astype(jnp.bfloat16)
            for part in (high, low):
                total += lax.dot_general(
                    part, rows[...], (((0,), (0,)), ((), ())), preferred_element_type=jnp.float32
                )
        out_ref[...] = total.astype(jnp.bfloat16)

    return pl.pallas_call(
        kernel,
        out_shape=jax.ShapeDtypeStruct((tokens, columns), jnp.bfloat16),
        name="combine",
    )(kept, *returned, *ranks, *shares)


def halves(value):
    high = value.astype(jnp.bfloat16)
    return high, (value - high.astype(jnp.float32)).astype(jnp.bfloat16)


def dot32(left, right):
    return jnp.dot(left, right, preferred_element_type=jnp.float32)


def to_channels(value, group, per_group, channels):
    heads = value.shape[1]
    row = lax.broadcasted_iota(jnp.int32, (heads, channels), 0)
    column = lax.broadcasted_iota(jnp.int32, (heads, channels), 1)
    spread = (row == group * per_group + column // (channels // per_group)).astype(jnp.bfloat16)
    high, low = halves(value)
    return dot32(high, spread) + dot32(low, spread)


def convolve(halo, rows, taps, scratch):
    lead, length = halo.shape[0], rows.shape[0]
    count = taps.shape[0]
    scratch[:lead] = halo[...].astype(jnp.float32)
    scratch[lead:] = rows[...].astype(jnp.float32)
    weights = taps[...].astype(jnp.float32)
    total = weights[0:1] * scratch[lead - count + 1 : lead - count + 1 + length]
    for k in range(1, count):
        total += weights[k : k + 1] * scratch[lead - count + 1 + k : lead - count + 1 + k + length]
    return silu(total)


def mixer_states(act, writes, halo, taps, write_taps, raw, bias, decay, groups, span):
    length, heads = raw.shape
    channels, state = act.shape[1] // groups, writes.shape[1] // groups
    per_group = heads // groups
    blocks = length // span
    lead = halo.shape[0]
    skip = act.shape[1] // state

    def kernel(act_ref, write_ref, halo_ref, halo_w_ref, taps_ref, taps_w_ref, raw_ref, bias_ref,
               decay_ref, value_ref, out_w_ref, cum_ref, sum_ref, enter_ref, close_ref, scale_ref,
               pad_ref, pad_w_ref):
        group = pl.program_id(0)

        @pl.when(group == 0)
        def _():
            x = raw_ref[...].astype(jnp.float32) + bias_ref[...]
            step = jnp.maximum(x, 0.0) + jnp.log1p(jnp.exp(-jnp.abs(x)))
            logs = step * -jnp.exp(decay_ref[...])
            row = lax.broadcasted_iota(jnp.int32, (span, span), 0)
            column = lax.broadcasted_iota(jnp.int32, (span, span), 1)
            below = (row >= column).astype(jnp.bfloat16)
            base = jnp.zeros((1, heads), jnp.float32)
            for b in range(blocks):
                part = logs[b * span : (b + 1) * span]
                high, low = halves(part)
                rest = (part - high.astype(jnp.float32) - low.astype(jnp.float32)).astype(jnp.bfloat16)
                cum = dot32(below, high) + dot32(below, low) + dot32(below, rest)
                cum_ref[b * span : (b + 1) * span] = cum
                sum_ref[b * span : (b + 1) * span] = cum + base
                scale_ref[b * span : (b + 1) * span] = step[b * span : (b + 1) * span] * jnp.exp(-cum)
                base = base + cum[span - 1 : span]

        values = convolve(halo_ref, act_ref, taps_ref, pad_ref)
        scaled = values * to_channels(scale_ref[...], group, per_group, channels)
        value_ref[...] = scaled.astype(jnp.bfloat16)
        out_w_ref[...] = convolve(halo_w_ref, write_ref, taps_w_ref, pad_w_ref).astype(jnp.bfloat16)
        carried = jnp.zeros((state, channels), jnp.float32)
        ends = to_channels(jnp.exp(cum_ref[...]), group, per_group, channels)
        for b in range(blocks):
            enter_ref[b * state : (b + 1) * state] = carried.astype(jnp.bfloat16)
            here = lax.dot_general(
                out_w_ref[b * span : (b + 1) * span], value_ref[b * span : (b + 1) * span],
                (((0,), (0,)), ((), ())), preferred_element_type=jnp.float32,
            )
            carried = ends[(b + 1) * span - 1 : (b + 1) * span] * (carried + here)
        close_ref[:state] = carried.astype(jnp.bfloat16)
        total = to_channels(jnp.exp(sum_ref[length - 16 :]), group, per_group, channels)
        close_ref[state:] = jnp.broadcast_to(total[15:16], (16, channels)).astype(jnp.bfloat16)

    by_group = lambda rows, width: pl.BlockSpec((rows, width), lambda g: (0, g))
    whole = lambda rows, width: pl.BlockSpec((rows, width), lambda g: (0, 0))
    return pl.pallas_call(
        kernel,
        grid=(groups,),
        in_specs=[
            by_group(length, channels), by_group(length, state),
            by_group(lead, channels), pl.BlockSpec((lead, state), lambda g: (0, skip + g)),
            by_group(taps.shape[0], channels), by_group(taps.shape[0], state),
            whole(length, heads), whole(1, heads), whole(1, heads),
        ],
        out_specs=[
            by_group(length, channels), by_group(length, state), whole(length, heads),
            whole(length, heads), by_group(blocks * state, channels), by_group(state + 16, channels),
        ],
        out_shape=[
            jax.ShapeDtypeStruct((length, groups * channels), jnp.bfloat16),
            jax.ShapeDtypeStruct((length, groups * state), jnp.bfloat16),
            jax.ShapeDtypeStruct((length, heads), jnp.float32),
            jax.ShapeDtypeStruct((length, heads), jnp.float32),
            jax.ShapeDtypeStruct((blocks * state, groups * channels), jnp.bfloat16),
            jax.ShapeDtypeStruct((state + 16, groups * channels), jnp.bfloat16),
        ],
        scratch_shapes=[
            pltpu.VMEM((length, heads), jnp.float32),
            pltpu.VMEM((lead + length, channels), jnp.float32),
            pltpu.VMEM((lead + length, state), jnp.float32),
        ],
        compiler_params=pltpu.CompilerParams(dimension_semantics=("arbitrary",)),
        name="mixer_states",
    )(act, writes, halo, halo, taps, write_taps, raw, bias, decay)


def mixer_local(reads, halo, read_taps, values, writes, entering, cum, groups, span):
    length, heads = cum.shape
    channels, state = values.shape[1] // groups, reads.shape[1] // groups
    per_group = heads // groups
    blocks = length // span
    lead = halo.shape[0]
    skip = values.shape[1] // state + groups

    def kernel(read_ref, halo_ref, taps_ref, value_ref, write_ref, enter_ref, cum_ref, out_ref,
               out_r_ref, pad_ref):
        group = pl.program_id(0)
        out_r_ref[...] = convolve(halo_ref, read_ref, taps_ref, pad_ref).astype(jnp.bfloat16)
        grown = to_channels(jnp.exp(cum_ref[...]), group, per_group, channels)
        row = lax.broadcasted_iota(jnp.int32, (span, span), 0)
        column = lax.broadcasted_iota(jnp.int32, (span, span), 1)
        for b in range(blocks):
            at = slice(b * span, (b + 1) * span)
            meet = lax.dot_general(
                out_r_ref[at], write_ref[at], (((1,), (1,)), ((), ())),
                preferred_element_type=jnp.float32,
            )
            meet = jnp.where(row >= column, meet, 0.0).astype(jnp.bfloat16)
            total = dot32(meet, value_ref[at])
            if b:
                total += dot32(out_r_ref[at], enter_ref[b * state : (b + 1) * state])
            out_ref[at] = grown[at] * total

    by_group = lambda rows, width: pl.BlockSpec((rows, width), lambda g: (0, g))
    return pl.pallas_call(
        kernel,
        grid=(groups,),
        in_specs=[
            by_group(length, state), pl.BlockSpec((lead, state), lambda g: (0, skip + g)),
            by_group(read_taps.shape[0], state), by_group(length, channels),
            by_group(length, state), by_group(blocks * state, channels),
            pl.BlockSpec((length, heads), lambda g: (0, 0)),
        ],
        out_specs=[by_group(length, channels), by_group(length, state)],
        out_shape=[
            jax.ShapeDtypeStruct((length, groups * channels), jnp.float32),
            jax.ShapeDtypeStruct((length, groups * state), jnp.bfloat16),
        ],
        scratch_shapes=[pltpu.VMEM((lead + length, state), jnp.float32)],
        compiler_params=pltpu.CompilerParams(dimension_semantics=("arbitrary",)),
        cost_estimate=pl.CostEstimate(
            flops=4 * 10**9, bytes_accessed=4 * 10**6, transcendentals=length * groups * state
        ),
        name="mixer_local",
    )(reads, halo, read_taps, values, writes, entering, cum)


def mixer_project(local, reads, sums, arriving, gates, gain, weight, own, shares, groups):
    length, heads = sums.shape
    channels, state = local.shape[1] // groups, reads.shape[1] // groups
    per_group = heads // groups
    width = weight.shape[1] // shares

    def kernel(own_ref, local_ref, read_ref, sum_ref, arrive_ref, gate_ref, gain_ref, *refs):
        weights, outs, totals = refs[:shares], refs[shares : 2 * shares], refs[2 * shares :]
        group = pl.program_id(0)
        grown = to_channels(jnp.exp(sum_ref[...]), group, per_group, channels)
        y = local_ref[...] + grown * dot32(read_ref[...], arrive_ref[...])
        gated = y * silu(gate_ref[...].astype(jnp.float32))
        row = lax.broadcasted_iota(jnp.int32, (channels, channels), 0) // (channels // per_group)
        column = lax.broadcasted_iota(jnp.int32, (channels, channels), 1) // (channels // per_group)
        same = jnp.where(row == column, per_group / channels, 0.0).astype(jnp.bfloat16)
        high, low = halves(gated * gated)
        mean = dot32(high, same) + dot32(low, same)
        mixed = (gated * lax.rsqrt(mean + EPS) * gain_ref[...]).astype(jnp.bfloat16)
        for m in range(shares):
            part = dot32(mixed, weights[m][...])
            if groups == 1:
                outs[m][...] = part.astype(jnp.bfloat16)
                continue

            @pl.when(group == 0)
            def _():
                totals[m][...] = part

            @pl.when((group > 0) & (group < groups - 1))
            def _():
                totals[m][...] += part

            @pl.when(group == groups - 1)
            def _():
                outs[m][...] = (totals[m][...] + part).astype(jnp.bfloat16)

    by_group = lambda rows, width: pl.BlockSpec((rows, width), lambda g, o: (0, g))
    whole = lambda rows, width: pl.BlockSpec((rows, width), lambda g, o: (0, 0))
    share = lambda m: pl.BlockSpec((channels, width), lambda g, o: (g, o[0] ^ m))
    return pl.pallas_call(
        kernel,
        grid_spec=pltpu.PrefetchScalarGridSpec(
            num_scalar_prefetch=1,
            grid=(groups,),
            in_specs=[
                by_group(length, channels), by_group(length, state), whole(length, heads),
                by_group(state, channels), by_group(length, channels), by_group(1, channels),
            ]
            + [share(m) for m in range(shares)],
            out_specs=[whole(length, width) for _ in range(shares)],
            scratch_shapes=[pltpu.VMEM((length, width), jnp.float32) for _ in range(shares)],
        ),
        out_shape=[jax.ShapeDtypeStruct((length, width), jnp.bfloat16) for _ in range(shares)],
        compiler_params=pltpu.CompilerParams(dimension_semantics=("arbitrary",)),
        name="mixer_project",
    )(own, local, reads, sums, arriving, gates, gain, *[weight] * shares)


def arriving_state(closing, state):
    core = lax.axis_index("sp") % 2
    count = lax.axis_size("sp")
    half = closing.shape[1] // 2
    other = swap_core(closing)
    part = lambda rows: lax.dynamic_slice_in_dim(rows, core * half, half, 1).astype(jnp.float32)
    mine, theirs = part(closing), part(other)
    early = jnp.where(core == 0, mine, theirs)
    late = jnp.where(core == 0, theirs, mine)
    decay = late[state : state + 1]
    chip = jnp.concatenate([early[:state] * decay + late[:state], early[state:] * decay], axis=0)
    chip = chip.astype(jnp.bfloat16)
    sent = [
        lax.ppermute(chip, "sp", [(i, i + 2 * k) for i in range(count - 2 * k)])
        for k in range(1, count // 2)
    ]
    total = jnp.zeros((state, half), jnp.float32)
    for rows in reversed(sent):
        rows = rows.astype(jnp.float32)
        total = rows[:state] + rows[state : state + 1] * total
    total = total.astype(jnp.bfloat16)
    swapped = swap_core(total)
    low = jnp.where(core == 0, total, swapped)
    high = jnp.where(core == 0, swapped, total)
    both = jnp.concatenate([low, high], axis=1)
    before = other.astype(jnp.float32)
    after = before[:state] + before[state : state + 1] * both.astype(jnp.float32)
    return jnp.where(core == 0, both, after.astype(jnp.bfloat16))


def per_device(
    stream,
    inner_act,
    gate_act,
    state_write,
    state_read,
    step_raw,
    conv_inner,
    conv_write,
    conv_read,
    step_bias,
    decay_log,
    inner_gain,
    out_weight,
    ffn_gain,
    expert_ids,
    expert_weights,
    expert_gate,
    expert_up,
    expert_down,
):
    length = inner_act.shape[0]
    heads_here = step_raw.shape[1]
    groups_here = state_write.shape[1]
    state_dim = state_write.shape[2]
    inner_width = inner_act.shape[1]
    write_width = groups_here * state_dim
    write_act = state_write.reshape(length, write_width)
    read_act = state_read.reshape(length, write_width)
    tail_rows = [a[length - LEAD :] for a in (inner_act, write_act, read_act)]
    halo = from_behind(jnp.concatenate(tail_rows, axis=1), "sp", 1)
    own_tp = lax.axis_index("tp")
    own_index = own_tp.astype(jnp.int32).reshape(1)
    tp_count = lax.axis_size("tp")
    values, writes, cum, sums, entering, closing = mixer_states(
        inner_act,
        write_act,
        halo,
        conv_inner,
        conv_write.reshape(-1, write_width),
        step_raw,
        step_bias[None],
        decay_log[None],
        groups_here,
        SPAN,
    )
    arriving = arriving_state(closing, state_dim)
    local, reads = mixer_local(
        read_act,
        halo,
        conv_read.reshape(-1, write_width),
        values,
        writes,
        entering,
        cum,
        groups_here,
        SPAN,
    )
    leaving = mixer_project(
        local,
        reads,
        sums,
        arriving,
        gate_act,
        inner_gain[None],
        out_weight,
        own_index,
        tp_count,
        groups_here,
    )
    full_width = out_weight.shape[1]
    local_experts = expert_gate.shape[0]
    out_width = expert_down.shape[2]
    chips = lax.axis_size("sp") // 2
    own_sp = lax.axis_index("sp")
    own_start = own_tp * out_width
    ids_own = expert_ids.T
    ids_pair = jnp.stack([ids_own, swap_core(ids_own)])
    ids_of = [ids_pair] + [move_chips(ids_pair, k) for k in range(1, chips)]
    arriving_ranks = [
        [ranks_of(ids_of[k][side], own_sp * local_experts, local_experts) for side in range(2)]
        for k in range(chips)
    ]
    weights_own = expert_weights.T
    leaving_ranks, leaving_shares = [], []
    for k in range(chips):
        for side in range(2):
            owner = ((own_sp + 2 * k) % (2 * chips)) ^ side
            first = owner * local_experts
            leaving_ranks.append(ranks_of(ids_own, first, local_experts))
            experts = first + jnp.arange(local_experts, dtype=jnp.int32)
            leaving_shares.append(
                sum(
                    jnp.where(ids_own[j][None, :] == experts[:, None], weights_own[j][None, :], 0.0)
                    for j in range(TOPK)
                )
            )
    projected = leaving[0].astype(jnp.float32)
    for part in [swap_tp(leaving[m], m) for m in reversed(range(1, tp_count))]:
        projected = projected + part.astype(jnp.float32)
    kept = lax.dynamic_slice_in_dim(stream, own_start, out_width, 1).astype(jnp.float32) + projected
    square_total = sum_tp(jnp.sum(kept * kept, axis=1))
    gain_share = lax.dynamic_slice_in_dim(ffn_gain, own_start, out_width, 0)
    scale_rows = lax.rsqrt(square_total / full_width + EPS)
    normed = (kept * scale_rows[:, None] * gain_share[None, :]).astype(jnp.bfloat16)
    current = [normed]
    for k in range(1, chips):
        current.append(move_chips(current[-1], 1))
    returned = []
    for first in range(0, chips, CHUNK):
        chunk = range(first, min(first + CHUNK, chips))
        blocks = [rows for k in chunk for rows in (current[k], swap_core(current[k]))]
        ranks = [arriving_ranks[k][side] for k in chunk for side in range(2)]
        picked = pick_rows(blocks, ranks).reshape(-1, out_width)
        hidden = hidden_units(gather_tp(picked), expert_gate, expert_up, own_index)
        given = expert_rows(gather_tp(hidden), expert_down, own_index)
        for i, k in enumerate(chunk):
            returned.append(move_chips(given[2 * i], -k) if k else given[0])
            returned.append(move_chips(given[2 * i + 1], -k, True))
    return combine(kept, returned, leaving_ranks, leaving_shares)


def solution(mesh):
    return jax.shard_map(
        per_device,
        mesh=mesh,
        in_specs=(
            P("sp", None),
            P("sp", "tp"),
            P("sp", "tp"),
            P("sp", "tp", None),
            P("sp", "tp", None),
            P("sp", "tp"),
            P(None, "tp"),
            P(None, "tp", None),
            P(None, "tp", None),
            P("tp"),
            P("tp"),
            P("tp"),
            P("tp", None),
            P(),
            P("sp", None),
            P("sp", None),
            P("sp", None, "tp"),
            P("sp", None, "tp"),
            P("sp", None, "tp"),
        ),
        out_specs=P("sp", "tp"),
        check_vma=False,
    )
```

```python
import jax
import jax.numpy as jnp
from jax import lax
from jax.experimental import pallas as pl
from jax.experimental.pallas import tpu as pltpu
from jax.sharding import PartitionSpec as P

SPAN = 128
LEAD = 16
TOPK = 2
CAP = 48


EPS = 1e-06


def from_behind(value, axis, steps):
    count = lax.axis_size(axis)
    first, last = (max(0, -steps), min(count, count - steps))
    return lax.ppermute(value, axis, [(source, source + steps) for source in range(first, last)])


def silu(x):
    return x * (0.5 * jnp.tanh(0.5 * x) + 0.5)


def swap_core(value):
    count = lax.axis_size("sp")
    return lax.ppermute(value, "sp", [(i, i ^ 1) for i in range(count)])


def move_chips(value, steps, cross=False):
    count = lax.axis_size("sp")
    return lax.ppermute(
        value, "sp", [(i, ((i + 2 * steps) % count) ^ int(cross)) for i in range(count)]
    )


def swap_tp(value, mask):
    count = lax.axis_size("tp")
    return lax.ppermute(value, "tp", [(i, i ^ mask) for i in range(count)])


def after(value, *others):
    return lax.optimization_barrier((value, *others))[0]


def start_gather(rows, mask):
    if lax.axis_size("tp") != 4:
        return None
    return swap_tp(rows, mask), swap_tp(rows, 3 - mask)


def end_gather(rows, near, mask, *earlier):
    count = lax.axis_size("tp")
    if count != 4:
        every = lax.all_gather(after(rows, *earlier), "tp")
        own = lax.axis_index("tp")
        return [lax.dynamic_index_in_dim(every, own ^ m, 0, False) for m in range(count)]
    far = swap_tp(after(near[0], *earlier) if earlier else near[0], 3 - mask)
    return [rows, near[0], near[1], far] if mask == 1 else [rows, near[1], near[0], far]


def routing_tables(ids, weights, own, experts):
    blocks = ids.shape[0] // TOPK
    tokens = ids.shape[1]
    shape = (blocks, experts, tokens)

    def kernel(own_ref, ids_ref, weight_ref, arrive_ref, leave_ref, share_ref):
        expert = lax.broadcasted_iota(jnp.int32, (experts, tokens), 0)
        first = own_ref[0] * experts
        named = []
        for b in range(blocks):
            rows = [ids_ref[TOPK * b + j : TOPK * b + j + 1] for j in range(TOPK)]
            named.append(sum((row == expert + first).astype(jnp.float32) for row in rows))
        own_rows = [ids_ref[j : j + 1] for j in range(TOPK)]
        for b in range(blocks):
            owner = ((own_ref[0] + 2 * (b // 2)) % blocks) ^ (b % 2)
            hits = [(row == expert + owner * experts).astype(jnp.float32) for row in own_rows]
            named.append(sum(hits))
            share_ref[b] = sum(hit * weight_ref[j : j + 1] for j, hit in enumerate(hits))
        every = jnp.concatenate(named, axis=0)
        row = lax.broadcasted_iota(jnp.int32, (tokens, tokens), 0)
        column = lax.broadcasted_iota(jnp.int32, (tokens, tokens), 1)
        slots = dot32(every.astype(jnp.bfloat16), (row < column).astype(jnp.bfloat16))
        slots = jnp.where(every > 0, slots.astype(jnp.int32), -1)
        for b in range(blocks):
            arrive_ref[b] = slots[b * experts : (b + 1) * experts]
            leave_ref[b] = slots[(blocks + b) * experts : (blocks + b + 1) * experts]

    return pl.pallas_call(
        kernel,
        in_specs=[
            pl.BlockSpec(memory_space=pltpu.SMEM), pl.BlockSpec(memory_space=pltpu.VMEM),
            pl.BlockSpec(memory_space=pltpu.VMEM),
        ],
        out_shape=[
            jax.ShapeDtypeStruct(shape, jnp.int32), jax.ShapeDtypeStruct(shape, jnp.int32),
            jax.ShapeDtypeStruct(shape, jnp.float32),
        ],
        name="routing_tables",
    )(own, ids, weights)


def pick_rows(blocks, ranks, places):
    experts = ranks.shape[1]
    tokens, width = blocks[0].shape
    count = len(blocks)

    def kernel(*refs):
        block_refs, rank_ref, out_ref = refs[:count], refs[count], refs[-1]
        slot = lax.broadcasted_iota(jnp.int32, (CAP, tokens), 0)
        for side, rows in enumerate(block_refs):
            rank = rank_ref[places[side]]
            chosen = jnp.concatenate(
                [(rank[e : e + 1, :] == slot).astype(jnp.float32) for e in range(experts)], axis=0
            ).astype(jnp.bfloat16)
            picked = dot32(chosen, rows[...]).astype(jnp.bfloat16)
            for e in range(experts):
                out_ref[e, side] = picked[e * CAP : (e + 1) * CAP]

    return pl.pallas_call(
        kernel,
        out_shape=jax.ShapeDtypeStruct((experts, count, CAP, width), jnp.bfloat16),
        cost_estimate=pl.CostEstimate(
            flops=2 * count * experts * CAP * tokens * width,
            bytes_accessed=4 * count * tokens * width,
            transcendentals=0,
        ),
        name="pick_rows",
    )(*blocks, ranks)


def hidden_units(pieces, gate, up, inverse, own):
    experts, full, units = gate.shape
    rows, width = pieces[0].shape
    each = rows // experts
    count = len(pieces)
    lanes = inverse.shape[1]

    def kernel(own_ref, *refs):
        parts, (gate_ref, up_ref, inverse_ref, out_ref) = refs[:count], refs[count:]
        gate_sum = jnp.zeros((each, units), jnp.float32)
        up_sum = jnp.zeros((each, units), jnp.float32)
        squares = jnp.zeros((each, lanes), jnp.float32)
        for m in range(count):
            part = parts[m][...]
            at = pl.ds(pl.multiple_of((own_ref[0] ^ m) * width, width), width)
            gate_sum += dot32(part, gate_ref[0, at, :])
            up_sum += dot32(part, up_ref[0, at, :])
            squares += dot32(part * part, inverse_ref[at, :])
        scale = lax.rsqrt(squares[:, :1] / full + EPS)
        out_ref[...] = (silu(gate_sum * scale) * (up_sum * scale)).astype(jnp.bfloat16)

    return pl.pallas_call(
        kernel,
        grid_spec=pltpu.PrefetchScalarGridSpec(
            num_scalar_prefetch=1,
            grid=(experts,),
            in_specs=[pl.BlockSpec((each, width), lambda e, o: (e, 0)) for _ in range(count)]
            + [pl.BlockSpec((1, full, units), lambda e, o: (e, 0, 0)) for _ in range(2)]
            + [pl.BlockSpec((full, lanes), lambda e, o: (0, 0))],
            out_specs=pl.BlockSpec((each, units), lambda e, o: (e, 0)),
        ),
        out_shape=jax.ShapeDtypeStruct((rows, units), jnp.bfloat16),
        cost_estimate=pl.CostEstimate(
            flops=4 * rows * full * units,
            bytes_accessed=4 * experts * full * units,
            transcendentals=rows * units,
        ),
        name="hidden_units",
    )(own, *pieces, gate, up, inverse)


def expert_rows(pieces, down, own):
    experts, full, columns = down.shape
    rows, units = pieces[0].shape
    each = rows // experts
    blocks = each // CAP
    count = len(pieces)

    def kernel(own_ref, *refs):
        parts, down_ref, outs = refs[:count], refs[count], refs[count + 1 :]
        total = jnp.zeros((each, columns), jnp.float32)
        for m in range(count):
            at = pl.ds(pl.multiple_of((own_ref[0] ^ m) * units, units), units)
            total += dot32(parts[m][...], down_ref[0, at, :])
        for i in range(blocks):
            outs[i][...] = total[i * CAP : (i + 1) * CAP].astype(jnp.bfloat16)

    return pl.pallas_call(
        kernel,
        grid_spec=pltpu.PrefetchScalarGridSpec(
            num_scalar_prefetch=1,
            grid=(experts,),
            in_specs=[pl.BlockSpec((each, units), lambda e, o: (e, 0)) for _ in range(count)]
            + [pl.BlockSpec((1, full, columns), lambda e, o: (e, 0, 0))],
            out_specs=[pl.BlockSpec((CAP, columns), lambda e, o: (e, 0)) for _ in range(blocks)],
        ),
        out_shape=[jax.ShapeDtypeStruct((experts * CAP, columns), jnp.bfloat16) for _ in range(blocks)],
        cost_estimate=pl.CostEstimate(
            flops=2 * rows * full * columns,
            bytes_accessed=2 * experts * full * columns,
            transcendentals=0,
        ),
        name="expert_rows",
    )(own, *pieces, down)


def combine(total, returned, places, ranks, shares, kind):
    tokens, columns = total.shape
    count = len(returned)
    experts = ranks.shape[1]

    def kernel(total_ref, *refs):
        rows_refs, rank_ref, share_ref, out_ref = refs[:count], refs[-3], refs[-2], refs[-1]
        slot = lax.broadcasted_iota(jnp.int32, (CAP, tokens), 0)
        value = total_ref[...]
        for place, rows in zip(places, rows_refs):
            rank, share = rank_ref[place], share_ref[place]
            chosen = jnp.concatenate(
                [
                    jnp.where(rank[e : e + 1, :] == slot, share[e : e + 1, :], 0.0)
                    for e in range(experts)
                ],
                axis=0,
            )
            for part in halves(chosen):
                value += lax.dot_general(
                    part, rows[...], (((0,), (0,)), ((), ())), preferred_element_type=jnp.float32
                )
        out_ref[...] = value.astype(kind)

    return pl.pallas_call(
        kernel,
        out_shape=jax.ShapeDtypeStruct((tokens, columns), kind),
        cost_estimate=pl.CostEstimate(
            flops=4 * count * tokens * experts * CAP * columns,
            bytes_accessed=8 * tokens * columns,
            transcendentals=0,
        ),
        name="combine",
    )(total, *returned, ranks, shares)


def halves(value):
    high = value.astype(jnp.bfloat16)
    return high, (value - high.astype(jnp.float32)).astype(jnp.bfloat16)


def dot32(left, right):
    return jnp.dot(left, right, preferred_element_type=jnp.float32)


def to_channels(value, group, per_group, channels):
    heads = value.shape[0]
    row = lax.broadcasted_iota(jnp.int32, (heads, channels), 0)
    column = lax.broadcasted_iota(jnp.int32, (heads, channels), 1)
    spread = (row == group * per_group + column // (channels // per_group)).astype(jnp.bfloat16)
    high, low = halves(value)
    over = (((0,), (0,)), ((), ()))
    return lax.dot_general(
        high, spread, over, preferred_element_type=jnp.float32
    ) + lax.dot_general(low, spread, over, preferred_element_type=jnp.float32)


def convolve(halo, rows, taps, scratch):
    lead, length = halo.shape[0], rows.shape[0]
    count = taps.shape[0]
    scratch[:lead] = halo[...].astype(jnp.float32)
    scratch[lead:] = rows[...].astype(jnp.float32)
    weights = taps[...].astype(jnp.float32)
    total = weights[0:1] * scratch[lead - count + 1 : lead - count + 1 + length]
    for k in range(1, count):
        total += weights[k : k + 1] * scratch[lead - count + 1 + k : lead - count + 1 + k + length]
    return silu(total)


def mixer_states(act, writes, halo, taps, write_taps, raw, bias, decay, groups, span):
    heads, length = raw.shape
    channels, state = act.shape[1] // groups, writes.shape[2]
    per_group = heads // groups
    blocks = length // span
    lead = halo.shape[0]
    skip = act.shape[1] // state

    def kernel(act_ref, write_ref, halo_ref, halo_w_ref, taps_ref, taps_w_ref, raw_ref, bias_ref,
               decay_ref, value_ref, out_w_ref, cum_ref, sum_ref, enter_ref, close_ref, scale_ref,
               pad_ref, pad_w_ref):
        group = pl.program_id(0)

        @pl.when(group == 0)
        def _():
            x = raw_ref[...].astype(jnp.float32) + bias_ref[...]
            step = jnp.maximum(x, 0.0) + jnp.log1p(jnp.exp(-jnp.abs(x)))
            logs = step * -jnp.exp(decay_ref[...])
            row = lax.broadcasted_iota(jnp.int32, (span, span), 0)
            column = lax.broadcasted_iota(jnp.int32, (span, span), 1)
            upto = (row <= column).astype(jnp.bfloat16)
            base = jnp.zeros((heads, 1), jnp.float32)
            for b in range(blocks):
                at = slice(b * span, (b + 1) * span)
                part = logs[:, at]
                high, low = halves(part)
                rest = (part - high.astype(jnp.float32) - low.astype(jnp.float32)).astype(jnp.bfloat16)
                cum = dot32(high, upto) + dot32(low, upto) + dot32(rest, upto)
                cum_ref[:, at] = cum
                sum_ref[:, at] = cum + base
                scale_ref[:, at] = step[:, at] * jnp.exp(-cum)
                base = base + cum[:, span - 1 : span]

        values = convolve(halo_ref, act_ref, taps_ref, pad_ref)
        scaled = values * to_channels(scale_ref[...], group, per_group, channels)
        value_ref[...] = scaled.astype(jnp.bfloat16)
        out_w_ref[...] = convolve(
            halo_w_ref, write_ref.at[0], taps_w_ref, pad_w_ref
        ).astype(jnp.bfloat16)
        carried = jnp.zeros((state, channels), jnp.float32)
        ends = to_channels(jnp.exp(cum_ref[...]), group, per_group, channels)
        for b in range(blocks):
            enter_ref[b * state : (b + 1) * state] = carried.astype(jnp.bfloat16)
            here = lax.dot_general(
                out_w_ref[b * span : (b + 1) * span], value_ref[b * span : (b + 1) * span],
                (((0,), (0,)), ((), ())), preferred_element_type=jnp.float32,
            )
            carried = ends[(b + 1) * span - 1 : (b + 1) * span] * (carried + here)
        close_ref[:state] = carried.astype(jnp.bfloat16)
        total = to_channels(jnp.exp(sum_ref[:, length - span :]), group, per_group, channels)
        close_ref[state:] = jnp.broadcast_to(total[span - 1 :], (16, channels)).astype(jnp.bfloat16)

    by_group = lambda rows, width: pl.BlockSpec((rows, width), lambda g: (0, g))
    whole = lambda rows, width: pl.BlockSpec((rows, width), lambda g: (0, 0))
    return pl.pallas_call(
        kernel,
        grid=(groups,),
        in_specs=[
            by_group(length, channels), pl.BlockSpec((1, length, state), lambda g: (g, 0, 0)),
            by_group(lead, channels), pl.BlockSpec((lead, state), lambda g: (0, skip + g)),
            by_group(taps.shape[0], channels), by_group(taps.shape[0], state),
            whole(heads, length), whole(heads, 1), whole(heads, 1),
        ],
        out_specs=[
            by_group(length, channels), by_group(length, state), whole(heads, length),
            whole(heads, length), by_group(blocks * state, channels), by_group(state + 16, channels),
        ],
        out_shape=[
            jax.ShapeDtypeStruct((length, groups * channels), jnp.bfloat16),
            jax.ShapeDtypeStruct((length, groups * state), jnp.bfloat16),
            jax.ShapeDtypeStruct((heads, length), jnp.float32),
            jax.ShapeDtypeStruct((heads, length), jnp.float32),
            jax.ShapeDtypeStruct((blocks * state, groups * channels), jnp.bfloat16),
            jax.ShapeDtypeStruct((state + 16, groups * channels), jnp.bfloat16),
        ],
        scratch_shapes=[
            pltpu.VMEM((heads, length), jnp.float32),
            pltpu.VMEM((lead + length, channels), jnp.float32),
            pltpu.VMEM((lead + length, state), jnp.float32),
        ],
        compiler_params=pltpu.CompilerParams(dimension_semantics=("arbitrary",)),
        name="mixer_states",
    )(act, writes, halo, halo, taps, write_taps, raw, bias, decay)


def mixer_local(reads, halo, read_taps, values, writes, entering, cum, groups, span):
    heads, length = cum.shape
    channels, state = values.shape[1] // groups, reads.shape[2]
    per_group = heads // groups
    blocks = length // span
    lead = halo.shape[0]
    skip = values.shape[1] // state + groups

    def kernel(read_ref, halo_ref, taps_ref, value_ref, write_ref, enter_ref, cum_ref, out_ref,
               out_r_ref, pad_ref):
        group = pl.program_id(0)
        out_r_ref[...] = convolve(halo_ref, read_ref.at[0], taps_ref, pad_ref).astype(jnp.bfloat16)
        grown = to_channels(jnp.exp(cum_ref[...]), group, per_group, channels)
        row = lax.broadcasted_iota(jnp.int32, (span, span), 0)
        column = lax.broadcasted_iota(jnp.int32, (span, span), 1)
        for b in range(blocks):
            at = slice(b * span, (b + 1) * span)
            meet = lax.dot_general(
                out_r_ref[at], write_ref[at], (((1,), (1,)), ((), ())),
                preferred_element_type=jnp.float32,
            )
            meet = jnp.where(row >= column, meet, 0.0).astype(jnp.bfloat16)
            total = dot32(meet, value_ref[at])
            if b:
                total += dot32(out_r_ref[at], enter_ref[b * state : (b + 1) * state])
            out_ref[at] = grown[at] * total

    by_group = lambda rows, width: pl.BlockSpec((rows, width), lambda g: (0, g))
    return pl.pallas_call(
        kernel,
        grid=(groups,),
        in_specs=[
            pl.BlockSpec((1, length, state), lambda g: (g, 0, 0)),
            pl.BlockSpec((lead, state), lambda g: (0, skip + g)), by_group(read_taps.shape[0], state), by_group(length, channels),
            by_group(length, state), by_group(blocks * state, channels),
            pl.BlockSpec((heads, length), lambda g: (0, 0)),
        ],
        out_specs=[by_group(length, channels), by_group(length, state)],
        out_shape=[
            jax.ShapeDtypeStruct((length, groups * channels), jnp.float32),
            jax.ShapeDtypeStruct((length, groups * state), jnp.bfloat16),
        ],
        scratch_shapes=[pltpu.VMEM((lead + length, state), jnp.float32)],
        compiler_params=pltpu.CompilerParams(dimension_semantics=("arbitrary",)),
        cost_estimate=pl.CostEstimate(
            flops=4 * 10**9, bytes_accessed=4 * 10**6, transcendentals=length * groups * state
        ),
        name="mixer_local",
    )(reads, halo, read_taps, values, writes, entering, cum)


def mixer_project(local, reads, sums, arriving, gates, gain, weight, own, shares, groups):
    heads, length = sums.shape
    channels, state = local.shape[1] // groups, reads.shape[1] // groups
    per_group = heads // groups
    width = weight.shape[1] // shares

    def kernel(own_ref, local_ref, read_ref, sum_ref, arrive_ref, gate_ref, gain_ref, *refs):
        weights, outs, mixed_ref = refs[:shares], refs[shares : 2 * shares], refs[-1]
        group = pl.program_id(0)
        grown = to_channels(jnp.exp(sum_ref[...]), group, per_group, channels)
        y = local_ref[...] + grown * dot32(read_ref[...], arrive_ref[...])
        gated = y * silu(gate_ref[...].astype(jnp.float32))
        row = lax.broadcasted_iota(jnp.int32, (channels, channels), 0) // (channels // per_group)
        column = lax.broadcasted_iota(jnp.int32, (channels, channels), 1) // (channels // per_group)
        same = jnp.where(row == column, per_group / channels, 0.0).astype(jnp.bfloat16)
        high, low = halves(gated * gated)
        mean = dot32(high, same) + dot32(low, same)
        mixed_ref[group] = (gated * lax.rsqrt(mean + EPS) * gain_ref[...]).astype(jnp.bfloat16)

        @pl.when(group == groups - 1)
        def _():
            mixed = jnp.concatenate([mixed_ref[g] for g in range(groups)], axis=1)
            for m in reversed(range(shares)):
                outs[m][...] = dot32(mixed, weights[m][...]).astype(jnp.bfloat16)

    by_group = lambda rows, width: pl.BlockSpec((rows, width), lambda g, o: (0, g))
    whole = lambda rows, width: pl.BlockSpec((rows, width), lambda g, o: (0, 0))
    share = lambda m: pl.BlockSpec((weight.shape[0], width), lambda g, o: (0, o[0] ^ m))
    return pl.pallas_call(
        kernel,
        grid_spec=pltpu.PrefetchScalarGridSpec(
            num_scalar_prefetch=1,
            grid=(groups,),
            in_specs=[
                by_group(length, channels), by_group(length, state), whole(heads, length),
                by_group(state, channels), by_group(length, channels), by_group(1, channels),
            ]
            + [share(m) for m in range(shares)],
            out_specs=[whole(length, width) for _ in range(shares)],
            scratch_shapes=[pltpu.VMEM((groups, length, channels), jnp.bfloat16)],
        ),
        out_shape=[jax.ShapeDtypeStruct((length, width), jnp.bfloat16) for _ in range(shares)],
        compiler_params=pltpu.CompilerParams(dimension_semantics=("arbitrary",)),
        name="mixer_project",
    )(own, local, reads, sums, arriving, gates, gain, *[weight] * shares)


def sent_states(closing, state):
    core = lax.axis_index("sp") % 2
    count = lax.axis_size("sp")
    half = closing.shape[1] // 2
    other = swap_core(closing)
    part = lambda rows: lax.dynamic_slice_in_dim(rows, core * half, half, 1).astype(jnp.float32)
    mine, theirs = part(closing), part(other)
    early = jnp.where(core == 0, mine, theirs)
    late = jnp.where(core == 0, theirs, mine)
    decay = late[state : state + 1]
    chip = jnp.concatenate([early[:state] * decay + late[:state], early[state:] * decay], axis=0)
    chip = chip.astype(jnp.bfloat16)
    sent = [
        lax.ppermute(chip, "sp", [(i, i + 2 * k) for i in range(count - 2 * k)])
        for k in range(1, count // 2)
    ]
    return sent, other


def arriving_state(sent, other, state):
    core = lax.axis_index("sp") % 2
    total = jnp.zeros((state, sent[0].shape[1]), jnp.float32)
    for rows in reversed(sent):
        rows = rows.astype(jnp.float32)
        total = rows[:state] + rows[state : state + 1] * total
    total = total.astype(jnp.bfloat16)
    swapped = swap_core(total)
    low = jnp.where(core == 0, total, swapped)
    high = jnp.where(core == 0, swapped, total)
    both = jnp.concatenate([low, high], axis=1)
    before = other.astype(jnp.float32)
    after = before[:state] + before[state : state + 1] * both.astype(jnp.float32)
    return jnp.where(core == 0, both, after.astype(jnp.bfloat16))


def per_device(
    stream,
    inner_act,
    gate_act,
    state_write,
    state_read,
    step_raw,
    conv_inner,
    conv_write,
    conv_read,
    step_bias,
    decay_log,
    inner_gain,
    out_weight,
    ffn_gain,
    expert_ids,
    expert_weights,
    expert_gate,
    expert_up,
    expert_down,
):
    length = inner_act.shape[0]
    heads_here = step_raw.shape[1]
    groups_here = state_write.shape[1]
    state_dim = state_write.shape[2]
    inner_width = inner_act.shape[1]
    write_width = groups_here * state_dim
    write_act = jnp.transpose(state_write, (1, 0, 2))
    read_act = jnp.transpose(state_read, (1, 0, 2))
    tail_rows = [inner_act[length - LEAD :]]
    tail_rows += [a[length - LEAD :].reshape(LEAD, write_width) for a in (state_write, state_read)]
    halo = from_behind(jnp.concatenate(tail_rows, axis=1), "sp", 1)
    own_tp = lax.axis_index("tp")
    own_sp = lax.axis_index("sp")
    own_index = own_tp.astype(jnp.int32).reshape(1)
    tp_count = lax.axis_size("tp")
    chips = lax.axis_size("sp") // 2
    values, writes, cum, sums, entering, closing = mixer_states(
        inner_act,
        write_act,
        halo,
        conv_inner,
        conv_write.reshape(-1, write_width),
        step_raw.T,
        step_bias[:, None],
        decay_log[:, None],
        groups_here,
        SPAN,
    )
    sent, other = sent_states(closing, state_dim)
    local, reads = mixer_local(
        read_act,
        halo,
        conv_read.reshape(-1, write_width),
        values,
        writes,
        entering,
        cum,
        groups_here,
        SPAN,
    )
    local_experts = expert_gate.shape[0]
    ids_own = expert_ids.T
    ids_pair = jnp.concatenate([ids_own, swap_core(ids_own)], axis=0)
    ids_of = [ids_pair] + [move_chips(ids_pair, k) for k in range(1, chips)]
    arrive_ranks, leave_ranks, shares = routing_tables(
        jnp.concatenate(ids_of, axis=0),
        expert_weights.T,
        own_sp.astype(jnp.int32).reshape(1),
        local_experts,
    )
    out_width = expert_down.shape[2]
    own_start = own_tp * out_width
    share_of = lax.dynamic_slice_in_dim(stream, own_start, out_width, 1)
    gain_share = lax.dynamic_slice_in_dim(ffn_gain, own_start, out_width, 0)
    inverse = jnp.broadcast_to((1.0 / (ffn_gain * ffn_gain))[:, None], (ffn_gain.shape[0], 128))
    inverse = inverse.astype(jnp.bfloat16)
    sent = [after(rows, local, arrive_ranks, share_of, inverse) for rows in sent]
    arriving = arriving_state(sent, other, state_dim)
    leaving = mixer_project(
        local,
        reads,
        sums,
        arriving,
        gate_act,
        inner_gain[None],
        out_weight,
        own_index,
        tp_count,
        groups_here,
    )
    projected = leaving[0].astype(jnp.float32)
    for part in [swap_tp(leaving[m], m) for m in reversed(range(1, tp_count))]:
        projected = projected + part.astype(jnp.float32)
    kept = share_of.astype(jnp.float32) + projected
    current = [(kept * gain_share[None, :]).astype(jnp.bfloat16)]
    chunks = [[0]] + [list(range(k, min(k + 2, chips))) for k in range(1, chips, 2)]
    count = len(chunks)
    picked, near, hidden, near_hidden, given, returned = [], [], [], [], [], []

    def give(i):
        mask = 1 + (i + 1) % 2
        earlier = given[-1:] and [given[-1][0]]
        pieces = end_gather(hidden[i], near_hidden[i], mask, *earlier)
        given.append(expert_rows(pieces, expert_down, own_index))
        for j, k in enumerate(chunks[i]):
            for side in range(2):
                rows = given[i][2 * j + side]
                home = rows if k == 0 and side == 0 else move_chips(rows, -k, bool(side))
                returned.append((2 * k + side, home))

    for i, chunk in enumerate(chunks):
        mask = 1 + i % 2
        blocks = []
        for k in chunk:
            if k:
                current.append(move_chips(after(current[-1], *picked[-1:]), 1))
            blocks += [current[k], swap_core(current[k])]
        rows = pick_rows(blocks, arrive_ranks, [2 * k + side for k in chunk for side in range(2)])
        rows = rows.reshape(-1, out_width)
        picked.append(after(rows, *near[-1]) if near and near[-1] else rows)
        near.append(start_gather(picked[i], mask))
        pieces = end_gather(picked[i], near[i], mask, *hidden[-1:])
        hidden.append(hidden_units(pieces, expert_gate, expert_up, inverse, own_index))
        near_hidden.append(start_gather(hidden[i], 3 - mask))
    for i in range(count):
        give(i)
    early = returned[: -2 * len(chunks[-1])]
    late = returned[-2 * len(chunks[-1]) :]
    total = combine(
        kept, [r for _, r in early], [p for p, _ in early], leave_ranks, shares, jnp.float32
    )
    return combine(
        total, [r for _, r in late], [p for p, _ in late], leave_ranks, shares, jnp.bfloat16
    )


def solution(mesh):
    return jax.shard_map(
        per_device,
        mesh=mesh,
        in_specs=(
            P("sp", None),
            P("sp", "tp"),
            P("sp", "tp"),
            P("sp", "tp", None),
            P("sp", "tp", None),
            P("sp", "tp"),
            P(None, "tp"),
            P(None, "tp", None),
            P(None, "tp", None),
            P("tp"),
            P("tp"),
            P("tp"),
            P("tp", None),
            P(),
            P("sp", None),
            P("sp", None),
            P("sp", None, "tp"),
            P("sp", None, "tp"),
            P("sp", None, "tp"),
        ),
        out_specs=P("sp", "tp"),
        check_vma=False,
    )
```

```python
import jax
import jax.numpy as jnp
from jax import lax
from jax.experimental import pallas as pl
from jax.experimental.pallas import tpu as pltpu
from jax.sharding import PartitionSpec as P

SPAN = 128
LEAD = 16
VMEM_LIMIT = 16 * 2**20
MIXER_LIMIT = 60 * 2**20
TOPK = 2
CAP = 48


EPS = 1e-06


def from_behind(value, axis, steps):
    count = lax.axis_size(axis)
    first, last = (max(0, -steps), min(count, count - steps))
    return lax.ppermute(value, axis, [(source, source + steps) for source in range(first, last)])


def silu(x):
    return x * (0.5 * jnp.tanh(0.5 * x) + 0.5)


def swap_core(value):
    count = lax.axis_size("sp")
    return lax.ppermute(value, "sp", [(i, i ^ 1) for i in range(count)])


def move_chips(value, steps, cross=False):
    count = lax.axis_size("sp")
    return lax.ppermute(
        value, "sp", [(i, ((i + 2 * steps) % count) ^ int(cross)) for i in range(count)]
    )


def swap_tp(value, mask):
    count = lax.axis_size("tp")
    return lax.ppermute(value, "tp", [(i, i ^ mask) for i in range(count)])


def gather_tp(rows, mask):
    count = lax.axis_size("tp")
    if count != 4:
        every = lax.all_gather(rows, "tp")
        own = lax.axis_index("tp")
        return [lax.dynamic_index_in_dim(every, own ^ m, 0, False) for m in range(count)]
    near = swap_tp(rows, mask)
    other = swap_tp(rows, 3 - mask)
    far = swap_tp(near, 3 - mask)
    return [rows, near, other, far] if mask == 1 else [rows, other, near, far]


def routing_tables(ids, weights, own, experts):
    blocks = ids.shape[0] // TOPK
    tokens = ids.shape[1]
    shape = (blocks, experts, tokens)

    def kernel(own_ref, ids_ref, weight_ref, arrive_ref, leave_ref, share_ref):
        expert = lax.broadcasted_iota(jnp.int32, (experts, tokens), 0)
        first = own_ref[0] * experts
        named = []
        for b in range(blocks):
            rows = [ids_ref[TOPK * b + j : TOPK * b + j + 1] for j in range(TOPK)]
            named.append(sum((row == expert + first).astype(jnp.float32) for row in rows))
        own_rows = [ids_ref[j : j + 1] for j in range(TOPK)]
        for b in range(blocks):
            owner = ((own_ref[0] + 2 * (b // 2)) % blocks) ^ (b % 2)
            hits = [(row == expert + owner * experts).astype(jnp.float32) for row in own_rows]
            named.append(sum(hits))
            share_ref[b] = sum(hit * weight_ref[j : j + 1] for j, hit in enumerate(hits))
        every = jnp.concatenate(named, axis=0)
        row = lax.broadcasted_iota(jnp.int32, (tokens, tokens), 0)
        column = lax.broadcasted_iota(jnp.int32, (tokens, tokens), 1)
        slots = dot32(every.astype(jnp.bfloat16), (row < column).astype(jnp.bfloat16))
        slots = jnp.where(every > 0, slots.astype(jnp.int32), -1)
        for b in range(blocks):
            arrive_ref[b] = slots[b * experts : (b + 1) * experts]
            leave_ref[b] = slots[(blocks + b) * experts : (blocks + b + 1) * experts]

    return pl.pallas_call(
        kernel,
        in_specs=[
            pl.BlockSpec(memory_space=pltpu.SMEM), pl.BlockSpec(memory_space=pltpu.VMEM),
            pl.BlockSpec(memory_space=pltpu.VMEM),
        ],
        out_shape=[
            jax.ShapeDtypeStruct(shape, jnp.int32), jax.ShapeDtypeStruct(shape, jnp.int32),
            jax.ShapeDtypeStruct(shape, jnp.float32),
        ],
        compiler_params=pltpu.CompilerParams(vmem_limit_bytes=VMEM_LIMIT),
        name="routing_tables",
    )(own, ids, weights)


def pick_rows(blocks, ranks, places):
    experts = ranks.shape[1]
    tokens, width = blocks[0].shape
    count = len(blocks)

    def kernel(*refs):
        block_refs, rank_ref, out_ref = refs[:count], refs[count], refs[-1]
        slot = lax.broadcasted_iota(jnp.int32, (CAP, tokens), 0)
        for side, rows in enumerate(block_refs):
            rank = rank_ref[places[side]]
            chosen = jnp.concatenate(
                [(rank[e : e + 1, :] == slot).astype(jnp.float32) for e in range(experts)], axis=0
            ).astype(jnp.bfloat16)
            picked = dot32(chosen, rows[...]).astype(jnp.bfloat16)
            for e in range(experts):
                out_ref[e, side] = picked[e * CAP : (e + 1) * CAP]

    return pl.pallas_call(
        kernel,
        out_shape=jax.ShapeDtypeStruct((experts, count, CAP, width), jnp.bfloat16),
        cost_estimate=pl.CostEstimate(
            flops=2 * count * experts * CAP * tokens * width,
            bytes_accessed=4 * count * tokens * width,
            transcendentals=0,
        ),
        compiler_params=pltpu.CompilerParams(vmem_limit_bytes=VMEM_LIMIT),
        name="pick_rows",
    )(*blocks, ranks)


def hidden_units(pieces, gate, up, inverse, own):
    experts, full, units = gate.shape
    rows, width = pieces[0].shape
    each = rows // experts
    count = len(pieces)
    lanes = inverse.shape[1]

    def kernel(own_ref, *refs):
        parts, (gate_ref, up_ref, inverse_ref, out_ref) = refs[:count], refs[count:]
        gate_sum = jnp.zeros((each, units), jnp.float32)
        up_sum = jnp.zeros((each, units), jnp.float32)
        squares = jnp.zeros((each, lanes), jnp.float32)
        for m in range(count):
            part = parts[m][...]
            at = pl.ds(pl.multiple_of((own_ref[0] ^ m) * width, width), width)
            gate_sum += dot32(part, gate_ref[0, at, :])
            up_sum += dot32(part, up_ref[0, at, :])
            squares += dot32(part * part, inverse_ref[at, :])
        scale = lax.rsqrt(squares[:, :1] / full + EPS)
        out_ref[...] = (silu(gate_sum * scale) * (up_sum * scale)).astype(jnp.bfloat16)

    return pl.pallas_call(
        kernel,
        grid_spec=pltpu.PrefetchScalarGridSpec(
            num_scalar_prefetch=1,
            grid=(experts,),
            in_specs=[pl.BlockSpec((each, width), lambda e, o: (e, 0)) for _ in range(count)]
            + [pl.BlockSpec((1, full, units), lambda e, o: (e, 0, 0)) for _ in range(2)]
            + [pl.BlockSpec((full, lanes), lambda e, o: (0, 0))],
            out_specs=pl.BlockSpec((each, units), lambda e, o: (e, 0)),
        ),
        out_shape=jax.ShapeDtypeStruct((rows, units), jnp.bfloat16),
        cost_estimate=pl.CostEstimate(
            flops=4 * rows * full * units,
            bytes_accessed=4 * experts * full * units,
            transcendentals=rows * units,
        ),
        compiler_params=pltpu.CompilerParams(vmem_limit_bytes=VMEM_LIMIT),
        name="hidden_units",
    )(own, *pieces, gate, up, inverse)


def expert_rows(pieces, down, own):
    experts, full, columns = down.shape
    rows, units = pieces[0].shape
    each = rows // experts
    blocks = each // CAP
    count = len(pieces)

    def kernel(own_ref, *refs):
        parts, down_ref, outs = refs[:count], refs[count], refs[count + 1 :]
        total = jnp.zeros((each, columns), jnp.float32)
        for m in range(count):
            at = pl.ds(pl.multiple_of((own_ref[0] ^ m) * units, units), units)
            total += dot32(parts[m][...], down_ref[0, at, :])
        for i in range(blocks):
            outs[i][...] = total[i * CAP : (i + 1) * CAP].astype(jnp.bfloat16)

    return pl.pallas_call(
        kernel,
        grid_spec=pltpu.PrefetchScalarGridSpec(
            num_scalar_prefetch=1,
            grid=(experts,),
            in_specs=[pl.BlockSpec((each, units), lambda e, o: (e, 0)) for _ in range(count)]
            + [pl.BlockSpec((1, full, columns), lambda e, o: (e, 0, 0))],
            out_specs=[pl.BlockSpec((CAP, columns), lambda e, o: (e, 0)) for _ in range(blocks)],
        ),
        out_shape=[jax.ShapeDtypeStruct((experts * CAP, columns), jnp.bfloat16) for _ in range(blocks)],
        cost_estimate=pl.CostEstimate(
            flops=2 * rows * full * columns,
            bytes_accessed=2 * experts * full * columns,
            transcendentals=0,
        ),
        compiler_params=pltpu.CompilerParams(vmem_limit_bytes=VMEM_LIMIT),
        name="expert_rows",
    )(own, *pieces, down)


def combine(total, returned, places, ranks, shares, kind):
    tokens, columns = total.shape
    count = len(returned)
    experts = ranks.shape[1]

    def kernel(total_ref, *refs):
        rows_refs, rank_ref, share_ref, out_ref = refs[:count], refs[-3], refs[-2], refs[-1]
        slot = lax.broadcasted_iota(jnp.int32, (CAP, tokens), 0)
        value = total_ref[...]
        for place, rows in zip(places, rows_refs):
            rank, share = rank_ref[place], share_ref[place]
            chosen = jnp.concatenate(
                [
                    jnp.where(rank[e : e + 1, :] == slot, share[e : e + 1, :], 0.0)
                    for e in range(experts)
                ],
                axis=0,
            )
            for part in halves(chosen):
                value += lax.dot_general(
                    part, rows[...], (((0,), (0,)), ((), ())), preferred_element_type=jnp.float32
                )
        out_ref[...] = value.astype(kind)

    return pl.pallas_call(
        kernel,
        out_shape=jax.ShapeDtypeStruct((tokens, columns), kind),
        cost_estimate=pl.CostEstimate(
            flops=4 * count * tokens * experts * CAP * columns,
            bytes_accessed=8 * tokens * columns,
            transcendentals=0,
        ),
        compiler_params=pltpu.CompilerParams(vmem_limit_bytes=VMEM_LIMIT),
        name="combine",
    )(total, *returned, ranks, shares)


def halves(value):
    high = value.astype(jnp.bfloat16)
    return high, (value - high.astype(jnp.float32)).astype(jnp.bfloat16)


def column(row):
    size = row.shape[1]
    same = lax.broadcasted_iota(jnp.int32, (size, size), 0) == lax.broadcasted_iota(
        jnp.int32, (size, size), 1
    )
    return jnp.sum(jnp.where(same, row, 0.0), axis=1, keepdims=True)


def dot32(left, right):
    return jnp.dot(left, right, preferred_element_type=jnp.float32)


def to_channels(value, group, per_group, channels):
    heads = value.shape[0]
    row = lax.broadcasted_iota(jnp.int32, (heads, channels), 0)
    column = lax.broadcasted_iota(jnp.int32, (heads, channels), 1)
    spread = (row == group * per_group + column // (channels // per_group)).astype(jnp.bfloat16)
    high, low = halves(value)
    over = (((0,), (0,)), ((), ()))
    return lax.dot_general(
        high, spread, over, preferred_element_type=jnp.float32
    ) + lax.dot_general(low, spread, over, preferred_element_type=jnp.float32)


def of_group(taps, group):
    place = lax.broadcasted_iota(jnp.int32, taps.shape, 1)
    return jnp.sum(jnp.where(place == group, taps[...].astype(jnp.float32), 0.0), axis=1)


def convolve(halo, rows, taps, scratch):
    lead, length = halo.shape[0], rows.shape[0]
    weights = taps.astype(jnp.float32)
    count = weights.shape[0]
    scratch[:lead] = halo[...].astype(jnp.float32)
    scratch[lead:] = rows[...].astype(jnp.float32)
    total = weights[0:1] * scratch[lead - count + 1 : lead - count + 1 + length]
    for k in range(1, count):
        total += weights[k : k + 1] * scratch[lead - count + 1 + k : lead - count + 1 + k + length]
    return silu(total)


def mixer_states(act, writes, halo, taps, write_taps, raw, bias, decay, groups, span):
    heads, length = raw.shape
    channels, state = act.shape[1] // groups, write_taps.shape[2]
    per_group = heads // groups
    blocks = length // span
    lead = halo.shape[0]
    skip = act.shape[1] // state

    def kernel(act_ref, write_ref, halo_ref, halo_w_ref, taps_ref, taps_w_ref, raw_ref, bias_ref,
               decay_ref, value_ref, out_w_ref, cum_ref, sum_ref, enter_ref, close_ref, scale_ref,
               pad_ref, pad_w_ref):
        group = pl.program_id(0)

        @pl.when(group == 0)
        def _():
            x = raw_ref[...].astype(jnp.float32) + column(bias_ref[...])
            step = jnp.maximum(x, 0.0) + jnp.log1p(jnp.exp(-jnp.abs(x)))
            logs = step * -jnp.exp(column(decay_ref[...]))
            row = lax.broadcasted_iota(jnp.int32, (span, span), 0)
            upto = (row <= lax.broadcasted_iota(jnp.int32, (span, span), 1)).astype(jnp.bfloat16)
            base = jnp.zeros((heads, 1), jnp.float32)
            for b in range(blocks):
                at = slice(b * span, (b + 1) * span)
                part = logs[:, at]
                high, low = halves(part)
                rest = (part - high.astype(jnp.float32) - low.astype(jnp.float32)).astype(jnp.bfloat16)
                cum = dot32(high, upto) + dot32(low, upto) + dot32(rest, upto)
                cum_ref[:, at] = cum
                sum_ref[:, at] = cum + base
                scale_ref[:, at] = step[:, at] * jnp.exp(-cum)
                base = base + cum[:, span - 1 : span]

        values = convolve(halo_ref, act_ref, taps_ref[...], pad_ref)
        scaled = values * to_channels(scale_ref[...], group, per_group, channels)
        value_ref[...] = scaled.astype(jnp.bfloat16)
        out_w_ref[...] = convolve(
            halo_w_ref, write_ref, of_group(taps_w_ref, group), pad_w_ref
        ).astype(jnp.bfloat16)
        carried = jnp.zeros((state, channels), jnp.float32)
        place = lax.broadcasted_iota(jnp.int32, (heads, 8), 1)
        lasts = sum_ref[:, length - 1 :]
        for b in range(blocks):
            lasts = jnp.where(place == b, cum_ref[:, (b + 1) * span - 1 : (b + 1) * span], lasts)
        ends = to_channels(jnp.exp(lasts), group, per_group, channels)
        for b in range(blocks):
            enter_ref[b * state : (b + 1) * state] = carried.astype(jnp.bfloat16)
            here = lax.dot_general(
                out_w_ref[b * span : (b + 1) * span], value_ref[b * span : (b + 1) * span],
                (((0,), (0,)), ((), ())), preferred_element_type=jnp.float32,
            )
            carried = ends[b : b + 1] * (carried + here)
        close_ref[:state] = carried.astype(jnp.bfloat16)
        close_ref[state:] = jnp.broadcast_to(ends[7:8], (16, channels)).astype(jnp.bfloat16)

    by_group = lambda rows, width: pl.BlockSpec((rows, width), lambda g: (0, g))
    whole = lambda rows, width: pl.BlockSpec((rows, width), lambda g: (0, 0))
    return pl.pallas_call(
        kernel,
        grid=(groups,),
        in_specs=[
            by_group(length, channels), by_group(length, state),
            by_group(lead, channels), pl.BlockSpec((lead, state), lambda g: (0, skip + g)),
            by_group(taps.shape[0], channels), pl.BlockSpec(write_taps.shape, lambda g: (0, 0, 0)),
            whole(heads, length), whole(1, heads), whole(1, heads),
        ],
        out_specs=[
            by_group(length, channels), by_group(length, state), whole(heads, length),
            whole(heads, length), by_group(blocks * state, channels), by_group(state + 16, channels),
        ],
        out_shape=[
            jax.ShapeDtypeStruct((length, groups * channels), jnp.bfloat16),
            jax.ShapeDtypeStruct((length, groups * state), jnp.bfloat16),
            jax.ShapeDtypeStruct((heads, length), jnp.float32),
            jax.ShapeDtypeStruct((heads, length), jnp.float32),
            jax.ShapeDtypeStruct((blocks * state, groups * channels), jnp.bfloat16),
            jax.ShapeDtypeStruct((state + 16, groups * channels), jnp.bfloat16),
        ],
        scratch_shapes=[
            pltpu.VMEM((heads, length), jnp.float32),
            pltpu.VMEM((lead + length, channels), jnp.float32),
            pltpu.VMEM((lead + length, state), jnp.float32),
        ],
        compiler_params=pltpu.CompilerParams(dimension_semantics=("arbitrary",), vmem_limit_bytes=MIXER_LIMIT),
        name="mixer_states",
    )(act, writes, halo, halo, taps, write_taps, raw, bias, decay)


def mixer_local(reads, halo, read_taps, values, writes, entering, cum, groups, span):
    heads, length = cum.shape
    channels, state = values.shape[1] // groups, read_taps.shape[2]
    per_group = heads // groups
    blocks = length // span
    lead = halo.shape[0]
    skip = values.shape[1] // state + groups

    def kernel(read_ref, halo_ref, taps_ref, value_ref, write_ref, enter_ref, cum_ref, out_ref,
               out_r_ref, pad_ref):
        group = pl.program_id(0)
        out_r_ref[...] = convolve(
            halo_ref, read_ref, of_group(taps_ref, group), pad_ref
        ).astype(jnp.bfloat16)
        grown = to_channels(jnp.exp(cum_ref[...]), group, per_group, channels)
        row = lax.broadcasted_iota(jnp.int32, (span, span), 0)
        column = lax.broadcasted_iota(jnp.int32, (span, span), 1)
        for b in range(blocks):
            at = slice(b * span, (b + 1) * span)
            meet = lax.dot_general(
                out_r_ref[at], write_ref[at], (((1,), (1,)), ((), ())),
                preferred_element_type=jnp.float32,
            )
            meet = jnp.where(row >= column, meet, 0.0).astype(jnp.bfloat16)
            total = dot32(meet, value_ref[at])
            if b:
                total += dot32(out_r_ref[at], enter_ref[b * state : (b + 1) * state])
            out_ref[at] = grown[at] * total

    by_group = lambda rows, width: pl.BlockSpec((rows, width), lambda g: (0, g))
    return pl.pallas_call(
        kernel,
        grid=(groups,),
        in_specs=[
            pl.BlockSpec((length, state), lambda g: (0, groups + g)),
            pl.BlockSpec((lead, state), lambda g: (0, skip + g)), pl.BlockSpec(read_taps.shape, lambda g: (0, 0, 0)), by_group(length, channels),
            by_group(length, state), by_group(blocks * state, channels),
            pl.BlockSpec((heads, length), lambda g: (0, 0)),
        ],
        out_specs=[by_group(length, channels), by_group(length, state)],
        out_shape=[
            jax.ShapeDtypeStruct((length, groups * channels), jnp.float32),
            jax.ShapeDtypeStruct((length, groups * state), jnp.bfloat16),
        ],
        scratch_shapes=[pltpu.VMEM((lead + length, state), jnp.float32)],
        compiler_params=pltpu.CompilerParams(dimension_semantics=("arbitrary",), vmem_limit_bytes=MIXER_LIMIT),
        cost_estimate=pl.CostEstimate(
            flops=4 * 10**9, bytes_accessed=4 * 10**6, transcendentals=length * groups * state
        ),
        name="mixer_local",
    )(reads, halo, read_taps, values, writes, entering, cum)


def mixer_project(local, reads, sums, arriving, gates, gain, weight, own, shares, groups):
    heads, length = sums.shape
    channels, state = local.shape[1] // groups, reads.shape[1] // groups
    per_group = heads // groups
    width = weight.shape[1] // shares

    def kernel(own_ref, local_ref, read_ref, sum_ref, arrive_ref, gate_ref, gain_ref, *refs):
        weights, outs = refs[:shares], refs[shares : 2 * shares]
        mixed_ref, kept_ref = refs[2 * shares :]
        group = pl.program_id(0)
        for m in range(shares):
            kept_ref[m, pl.ds(pl.multiple_of(group * channels, channels), channels)] = weights[m][...]
        grown = to_channels(jnp.exp(sum_ref[...]), group, per_group, channels)
        y = local_ref[...] + grown * dot32(read_ref[...], arrive_ref[...])
        gated = y * silu(gate_ref[...].astype(jnp.float32))
        row = lax.broadcasted_iota(jnp.int32, (channels, channels), 0) // (channels // per_group)
        column = lax.broadcasted_iota(jnp.int32, (channels, channels), 1) // (channels // per_group)
        same = jnp.where(row == column, per_group / channels, 0.0).astype(jnp.bfloat16)
        mean = dot32((gated * gated).astype(jnp.bfloat16), same)
        mixed_ref[group] = (gated * lax.rsqrt(mean + EPS) * gain_ref[...]).astype(jnp.bfloat16)

        @pl.when(group == groups - 1)
        def _():
            mixed = jnp.concatenate([mixed_ref[g] for g in range(groups)], axis=1)
            for m in reversed(range(shares)):
                outs[m][...] = dot32(mixed, kept_ref[m]).astype(jnp.bfloat16)

    by_group = lambda rows, width: pl.BlockSpec((rows, width), lambda g, o: (0, g))
    whole = lambda rows, width: pl.BlockSpec((rows, width), lambda g, o: (0, 0))
    share = lambda m: pl.BlockSpec((channels, width), lambda g, o: (g, o[0] ^ m))
    return pl.pallas_call(
        kernel,
        grid_spec=pltpu.PrefetchScalarGridSpec(
            num_scalar_prefetch=1,
            grid=(groups,),
            in_specs=[
                by_group(length, channels), by_group(length, state), whole(heads, length),
                by_group(state, channels), by_group(length, channels), by_group(1, channels),
            ]
            + [share(m) for m in range(shares)],
            out_specs=[whole(length, width) for _ in range(shares)],
            scratch_shapes=[
                pltpu.VMEM((groups, length, channels), jnp.bfloat16),
                pltpu.VMEM((shares, weight.shape[0], width), jnp.bfloat16),
            ],
        ),
        out_shape=[jax.ShapeDtypeStruct((length, width), jnp.bfloat16) for _ in range(shares)],
        compiler_params=pltpu.CompilerParams(dimension_semantics=("arbitrary",), vmem_limit_bytes=MIXER_LIMIT),
        name="mixer_project",
    )(own, local, reads, sums, arriving, gates, gain, *[weight] * shares)


def sent_states(closing, state):
    core = lax.axis_index("sp") % 2
    count = lax.axis_size("sp")
    half = closing.shape[1] // 2
    other = swap_core(closing)
    part = lambda rows: lax.dynamic_slice_in_dim(rows, core * half, half, 1).astype(jnp.float32)
    mine, theirs = part(closing), part(other)
    early = jnp.where(core == 0, mine, theirs)
    late = jnp.where(core == 0, theirs, mine)
    decay = late[state : state + 1]
    chip = jnp.concatenate([early[:state] * decay + late[:state], early[state:] * decay], axis=0)
    chip = chip.astype(jnp.bfloat16)
    sent = []
    for k in range(1, count // 2):
        pairs = [(i, i + 2 * k) for i in range(count - 2 * k)]
        sent.append(lax.ppermute(chip, "sp", pairs))
    return sent, other


def arriving_state(sent, other, state):
    core = lax.axis_index("sp") % 2
    total = jnp.zeros((state, sent[0].shape[1]), jnp.float32)
    for rows in reversed(sent):
        rows = rows.astype(jnp.float32)
        total = rows[:state] + rows[state : state + 1] * total
    total = total.astype(jnp.bfloat16)
    swapped = swap_core(total)
    low = jnp.where(core == 0, total, swapped)
    high = jnp.where(core == 0, swapped, total)
    both = jnp.concatenate([low, high], axis=1)
    before = other.astype(jnp.float32)
    after = before[:state] + before[state : state + 1] * both.astype(jnp.float32)
    return jnp.where(core == 0, both, after.astype(jnp.bfloat16))


def per_device(
    stream,
    inner_act,
    gate_act,
    state_write,
    state_read,
    step_raw,
    conv_inner,
    conv_write,
    conv_read,
    step_bias,
    decay_log,
    inner_gain,
    out_weight,
    ffn_gain,
    expert_ids,
    expert_weights,
    expert_gate,
    expert_up,
    expert_down,
):
    length = inner_act.shape[0]
    groups_here = state_write.shape[1]
    state_dim = state_write.shape[2]
    write_width = groups_here * state_dim
    tail_rows = [inner_act[length - LEAD :]]
    tail_rows += [a[length - LEAD :].reshape(LEAD, write_width) for a in (state_write, state_read)]
    halo = from_behind(jnp.concatenate(tail_rows, axis=1), "sp", 1)
    joined = jnp.concatenate(
        [a.reshape(length, write_width) for a in (state_write, state_read)], axis=1
    )
    own_tp = lax.axis_index("tp")
    own_sp = lax.axis_index("sp")
    own_index = own_tp.astype(jnp.int32).reshape(1)
    tp_count = lax.axis_size("tp")
    chips = lax.axis_size("sp") // 2
    values, writes, cum, sums, entering, closing = mixer_states(
        inner_act,
        joined,
        halo,
        conv_inner,
        conv_write,
        step_raw.T,
        step_bias[None],
        decay_log[None],
        groups_here,
        SPAN,
    )
    sent, other = sent_states(closing, state_dim)
    local, reads = mixer_local(
        joined,
        halo,
        conv_read,
        values,
        writes,
        entering,
        cum,
        groups_here,
        SPAN,
    )
    local_experts = expert_gate.shape[0]
    ids_own = expert_ids.T
    ids_other = swap_core(ids_own)
    ids_of = [jnp.concatenate([ids_own, ids_other], axis=0)]
    for k in range(1, chips):
        ids_of.append(move_chips(ids_of[0], k))
    arrive_ranks, leave_ranks, shares = routing_tables(
        jnp.concatenate(ids_of, axis=0),
        expert_weights.T,
        own_sp.astype(jnp.int32).reshape(1),
        local_experts,
    )
    out_width = expert_down.shape[2]
    own_start = own_tp * out_width
    share_of = lax.dynamic_slice_in_dim(stream, own_start, out_width, 1)
    gain_share = lax.dynamic_slice_in_dim(ffn_gain, own_start, out_width, 0)
    inverse = jnp.broadcast_to((1.0 / (ffn_gain * ffn_gain))[:, None], (ffn_gain.shape[0], 128))
    inverse = inverse.astype(jnp.bfloat16)
    arriving = arriving_state(sent, other, state_dim)
    leaving = mixer_project(
        local,
        reads,
        sums,
        arriving,
        gate_act,
        inner_gain[None],
        out_weight,
        own_index,
        tp_count,
        groups_here,
    )
    projected = leaving[0].astype(jnp.float32)
    for m in reversed(range(1, tp_count)):
        part = swap_tp(leaving[m], m)
        projected = projected + part.astype(jnp.float32)
    kept = share_of.astype(jnp.float32) + projected
    rows = (kept * gain_share[None, :]).astype(jnp.bfloat16)
    blocks_of = []
    for k in range(chips):
        if k:
            rows = move_chips(rows, 1)
        blocks_of.append([rows, swap_core(rows)])
    chunks = [[k] for k in range(chips)]
    returned = []
    for i, chunk in enumerate(chunks):
        mask, hidden_mask = RELAYS[i % 4]
        picked = pick_rows(
            [rows for k in chunk for rows in blocks_of[k]],
            arrive_ranks,
            [2 * k + side for k in chunk for side in range(2)],
        ).reshape(-1, out_width)
        pieces = gather_tp(picked, mask)
        hidden = hidden_units(pieces, expert_gate, expert_up, inverse, own_index)
        pieces = gather_tp(hidden, hidden_mask)
        given = expert_rows(pieces, expert_down, own_index)
        for j, k in enumerate(chunk):
            for side in range(2):
                home = given[2 * j + side]
                if k or side:
                    home = move_chips(home, -k, bool(side))
                returned.append((2 * k + side, home))
    returned = returned[2:-2] + returned[-2:] + returned[:2]
    late = 4
    total = kept
    for part, kind in ((returned[:-late], jnp.float32), (returned[-late:], jnp.bfloat16)):
        places, rows = zip(*part)
        total = combine(total, rows, places, leave_ranks, shares, kind)
    return total


RELAYS = ((2, 1), (1, 2), (2, 2), (1, 2))


def solution(mesh):
    return jax.shard_map(
        per_device,
        mesh=mesh,
        in_specs=(
            P("sp", None),
            P("sp", "tp"),
            P("sp", "tp"),
            P("sp", "tp", None),
            P("sp", "tp", None),
            P("sp", "tp"),
            P(None, "tp"),
            P(None, "tp", None),
            P(None, "tp", None),
            P("tp"),
            P("tp"),
            P("tp"),
            P("tp", None),
            P(),
            P("sp", None),
            P("sp", None),
            P("sp", None, "tp"),
            P("sp", None, "tp"),
            P("sp", None, "tp"),
        ),
        out_specs=P("sp", "tp"),
        check_vma=False,
    )
```

```python
import jax
import jax.numpy as jnp
from jax import lax
from jax.experimental import pallas as pl
from jax.experimental.pallas import tpu as pltpu
from jax.sharding import PartitionSpec as P

SPAN = 128
LEAD = 16
VMEM_LIMIT = 16 * 2**20
MIXER_LIMIT = 60 * 2**20
TOPK = 2
CAP = 48


EPS = 1e-06


def from_behind(value, axis, steps):
    count = lax.axis_size(axis)
    first, last = (max(0, -steps), min(count, count - steps))
    return lax.ppermute(value, axis, [(source, source + steps) for source in range(first, last)])


def silu(x):
    return x * (0.5 * jnp.tanh(0.5 * x) + 0.5)


def swap_core(value):
    count = lax.axis_size("sp")
    return lax.ppermute(value, "sp", [(i, i ^ 1) for i in range(count)])


def move_chips(value, steps, cross=False):
    count = lax.axis_size("sp")
    return lax.ppermute(
        value, "sp", [(i, ((i + 2 * steps) % count) ^ int(cross)) for i in range(count)]
    )


def swap_tp(value, mask):
    count = lax.axis_size("tp")
    return lax.ppermute(value, "tp", [(i, i ^ mask) for i in range(count)])


def gather_tp(rows, mask):
    count = lax.axis_size("tp")
    if count != 4:
        every = lax.all_gather(rows, "tp")
        own = lax.axis_index("tp")
        return [lax.dynamic_index_in_dim(every, own ^ m, 0, False) for m in range(count)]
    near = swap_tp(rows, mask)
    other = swap_tp(rows, 3 - mask)
    far = swap_tp(near, 3 - mask)
    return [rows, near, other, far] if mask == 1 else [rows, other, near, far]


def routing_tables(ids, weights, own, experts):
    blocks = ids.shape[0] // TOPK
    tokens = ids.shape[1]
    shape = (blocks, experts, tokens)

    def kernel(own_ref, ids_ref, weight_ref, arrive_ref, leave_ref, share_ref):
        expert = lax.broadcasted_iota(jnp.int32, (experts, tokens), 0)
        first = own_ref[0] * experts
        named = []
        for b in range(blocks):
            rows = [ids_ref[TOPK * b + j : TOPK * b + j + 1] for j in range(TOPK)]
            named.append(sum((row == expert + first).astype(jnp.float32) for row in rows))
        own_rows = [ids_ref[j : j + 1] for j in range(TOPK)]
        for b in range(blocks):
            owner = ((own_ref[0] + 2 * (b // 2)) % blocks) ^ (b % 2)
            hits = [(row == expert + owner * experts).astype(jnp.float32) for row in own_rows]
            named.append(sum(hits))
            share_ref[b] = sum(hit * weight_ref[j : j + 1] for j, hit in enumerate(hits))
        every = jnp.concatenate(named, axis=0)
        row = lax.broadcasted_iota(jnp.int32, (tokens, tokens), 0)
        column = lax.broadcasted_iota(jnp.int32, (tokens, tokens), 1)
        slots = dot32(every.astype(jnp.bfloat16), (row < column).astype(jnp.bfloat16))
        slots = jnp.where(every > 0, slots.astype(jnp.int32), -1)
        for b in range(blocks):
            arrive_ref[b] = slots[b * experts : (b + 1) * experts]
            leave_ref[b] = slots[(blocks + b) * experts : (blocks + b + 1) * experts]

    return pl.pallas_call(
        kernel,
        in_specs=[
            pl.BlockSpec(memory_space=pltpu.SMEM), pl.BlockSpec(memory_space=pltpu.VMEM),
            pl.BlockSpec(memory_space=pltpu.VMEM),
        ],
        out_shape=[
            jax.ShapeDtypeStruct(shape, jnp.int32), jax.ShapeDtypeStruct(shape, jnp.int32),
            jax.ShapeDtypeStruct(shape, jnp.float32),
        ],
        compiler_params=pltpu.CompilerParams(vmem_limit_bytes=VMEM_LIMIT),
        name="routing_tables",
    )(own, ids, weights)


def pick_rows(blocks, ranks, places):
    experts = ranks.shape[1]
    tokens, width = blocks[0].shape
    count = len(blocks)

    def kernel(*refs):
        block_refs, rank_ref, out_ref = refs[:count], refs[count], refs[-1]
        slot = lax.broadcasted_iota(jnp.int32, (CAP, tokens), 0)
        for side, rows in enumerate(block_refs):
            rank = rank_ref[places[side]]
            chosen = jnp.concatenate(
                [(rank[e : e + 1, :] == slot).astype(jnp.float32) for e in range(experts)], axis=0
            ).astype(jnp.bfloat16)
            picked = dot32(chosen, rows[...]).astype(jnp.bfloat16)
            for e in range(experts):
                out_ref[e, side] = picked[e * CAP : (e + 1) * CAP]

    return pl.pallas_call(
        kernel,
        out_shape=jax.ShapeDtypeStruct((experts, count, CAP, width), jnp.bfloat16),
        cost_estimate=pl.CostEstimate(
            flops=2 * count * experts * CAP * tokens * width,
            bytes_accessed=4 * count * tokens * width,
            transcendentals=0,
        ),
        compiler_params=pltpu.CompilerParams(vmem_limit_bytes=VMEM_LIMIT),
        name="pick_rows",
    )(*blocks, ranks)


def hidden_units(pieces, gate, up, inverse, own):
    experts, full, units = gate.shape
    rows, width = pieces[0].shape
    each = rows // experts
    count = len(pieces)
    lanes = inverse.shape[1]

    def kernel(own_ref, *refs):
        parts, (gate_ref, up_ref, inverse_ref, out_ref) = refs[:count], refs[count:]
        gate_sum = jnp.zeros((each, units), jnp.float32)
        up_sum = jnp.zeros((each, units), jnp.float32)
        squares = jnp.zeros((each, lanes), jnp.float32)
        for m in range(count):
            part = parts[m][...]
            at = pl.ds(pl.multiple_of((own_ref[0] ^ m) * width, width), width)
            gate_sum += dot32(part, gate_ref[0, at, :])
            up_sum += dot32(part, up_ref[0, at, :])
            squares += dot32(part * part, inverse_ref[at, :])
        scale = lax.rsqrt(squares[:, :1] / full + EPS)
        out_ref[...] = (silu(gate_sum * scale) * (up_sum * scale)).astype(jnp.bfloat16)

    return pl.pallas_call(
        kernel,
        grid_spec=pltpu.PrefetchScalarGridSpec(
            num_scalar_prefetch=1,
            grid=(experts,),
            in_specs=[pl.BlockSpec((each, width), lambda e, o: (e, 0)) for _ in range(count)]
            + [pl.BlockSpec((1, full, units), lambda e, o: (e, 0, 0)) for _ in range(2)]
            + [pl.BlockSpec((full, lanes), lambda e, o: (0, 0))],
            out_specs=pl.BlockSpec((each, units), lambda e, o: (e, 0)),
        ),
        out_shape=jax.ShapeDtypeStruct((rows, units), jnp.bfloat16),
        cost_estimate=pl.CostEstimate(
            flops=4 * rows * full * units,
            bytes_accessed=4 * experts * full * units,
            transcendentals=rows * units,
        ),
        compiler_params=pltpu.CompilerParams(vmem_limit_bytes=VMEM_LIMIT),
        name="hidden_units",
    )(own, *pieces, gate, up, inverse)


def expert_rows(pieces, down, own):
    experts, full, columns = down.shape
    rows, units = pieces[0].shape
    each = rows // experts
    blocks = each // CAP
    count = len(pieces)

    def kernel(own_ref, *refs):
        parts, down_ref, outs = refs[:count], refs[count], refs[count + 1 :]
        total = jnp.zeros((each, columns), jnp.float32)
        for m in range(count):
            at = pl.ds(pl.multiple_of((own_ref[0] ^ m) * units, units), units)
            total += dot32(parts[m][...], down_ref[0, at, :])
        for i in range(blocks):
            outs[i][...] = total[i * CAP : (i + 1) * CAP].astype(jnp.bfloat16)

    return pl.pallas_call(
        kernel,
        grid_spec=pltpu.PrefetchScalarGridSpec(
            num_scalar_prefetch=1,
            grid=(experts,),
            in_specs=[pl.BlockSpec((each, units), lambda e, o: (e, 0)) for _ in range(count)]
            + [pl.BlockSpec((1, full, columns), lambda e, o: (e, 0, 0))],
            out_specs=[pl.BlockSpec((CAP, columns), lambda e, o: (e, 0)) for _ in range(blocks)],
        ),
        out_shape=[jax.ShapeDtypeStruct((experts * CAP, columns), jnp.bfloat16) for _ in range(blocks)],
        cost_estimate=pl.CostEstimate(
            flops=2 * rows * full * columns,
            bytes_accessed=2 * experts * full * columns,
            transcendentals=0,
        ),
        compiler_params=pltpu.CompilerParams(vmem_limit_bytes=VMEM_LIMIT),
        name="expert_rows",
    )(own, *pieces, down)


def combine(total, returned, places, ranks, shares, kind):
    tokens, columns = total.shape
    count = len(returned)
    experts = ranks.shape[1]

    def kernel(total_ref, *refs):
        rows_refs, rank_ref, share_ref, out_ref = refs[:count], refs[-3], refs[-2], refs[-1]
        slot = lax.broadcasted_iota(jnp.int32, (CAP, tokens), 0)
        value = total_ref[...]
        for place, rows in zip(places, rows_refs):
            rank, share = rank_ref[place], share_ref[place]
            chosen = jnp.concatenate(
                [
                    jnp.where(rank[e : e + 1, :] == slot, share[e : e + 1, :], 0.0)
                    for e in range(experts)
                ],
                axis=0,
            )
            for part in halves(chosen):
                value += lax.dot_general(
                    part, rows[...], (((0,), (0,)), ((), ())), preferred_element_type=jnp.float32
                )
        out_ref[...] = value.astype(kind)

    return pl.pallas_call(
        kernel,
        out_shape=jax.ShapeDtypeStruct((tokens, columns), kind),
        cost_estimate=pl.CostEstimate(
            flops=4 * count * tokens * experts * CAP * columns,
            bytes_accessed=8 * tokens * columns,
            transcendentals=0,
        ),
        compiler_params=pltpu.CompilerParams(vmem_limit_bytes=VMEM_LIMIT),
        name="combine",
    )(total, *returned, ranks, shares)


def halves(value):
    high = value.astype(jnp.bfloat16)
    return high, (value - high.astype(jnp.float32)).astype(jnp.bfloat16)


def column(row):
    size = row.shape[1]
    same = lax.broadcasted_iota(jnp.int32, (size, size), 0) == lax.broadcasted_iota(
        jnp.int32, (size, size), 1
    )
    return jnp.sum(jnp.where(same, row, 0.0), axis=1, keepdims=True)


def dot32(left, right):
    return jnp.dot(left, right, preferred_element_type=jnp.float32)


def to_channels(value, group, per_group, channels):
    heads = value.shape[0]
    row = lax.broadcasted_iota(jnp.int32, (heads, channels), 0)
    column = lax.broadcasted_iota(jnp.int32, (heads, channels), 1)
    spread = (row == group * per_group + column // (channels // per_group)).astype(jnp.bfloat16)
    high, low = halves(value)
    over = (((0,), (0,)), ((), ()))
    return lax.dot_general(
        high, spread, over, preferred_element_type=jnp.float32
    ) + lax.dot_general(low, spread, over, preferred_element_type=jnp.float32)


def of_group(taps, group):
    place = lax.broadcasted_iota(jnp.int32, taps.shape, 1)
    return jnp.sum(jnp.where(place == group, taps[...].astype(jnp.float32), 0.0), axis=1)


def convolve(halo, rows, taps, scratch):
    lead, length = halo.shape[0], rows.shape[0]
    weights = taps.astype(jnp.float32)
    count = weights.shape[0]
    scratch[:lead] = halo[...].astype(jnp.float32)
    scratch[lead:] = rows[...].astype(jnp.float32)
    total = weights[0:1] * scratch[lead - count + 1 : lead - count + 1 + length]
    for k in range(1, count):
        total += weights[k : k + 1] * scratch[lead - count + 1 + k : lead - count + 1 + k + length]
    return silu(total)


def mixer_states(act, writes, halo, taps, write_taps, raw, bias, decay, groups, span):
    heads, length = raw.shape
    channels, state = act.shape[1] // groups, write_taps.shape[2]
    per_group = heads // groups
    blocks = length // span
    lead = halo.shape[0]
    skip = act.shape[1] // state

    def kernel(act_ref, write_ref, halo_ref, halo_w_ref, taps_ref, taps_w_ref, raw_ref, bias_ref,
               decay_ref, value_ref, out_w_ref, cum_ref, sum_ref, enter_ref, close_ref, scale_ref,
               pad_ref, pad_w_ref):
        group = pl.program_id(0)

        @pl.when(group == 0)
        def _():
            x = raw_ref[...].astype(jnp.float32) + column(bias_ref[...])
            step = jnp.maximum(x, 0.0) + jnp.log1p(jnp.exp(-jnp.abs(x)))
            logs = step * -jnp.exp(column(decay_ref[...]))
            row = lax.broadcasted_iota(jnp.int32, (span, span), 0)
            upto = (row <= lax.broadcasted_iota(jnp.int32, (span, span), 1)).astype(jnp.bfloat16)
            base = jnp.zeros((heads, 1), jnp.float32)
            for b in range(blocks):
                at = slice(b * span, (b + 1) * span)
                part = logs[:, at]
                high, low = halves(part)
                rest = (part - high.astype(jnp.float32) - low.astype(jnp.float32)).astype(jnp.bfloat16)
                cum = dot32(high, upto) + dot32(low, upto) + dot32(rest, upto)
                cum_ref[:, at] = cum
                sum_ref[:, at] = cum + base
                scale_ref[:, at] = step[:, at] * jnp.exp(-cum)
                base = base + cum[:, span - 1 : span]

        values = convolve(halo_ref, act_ref, taps_ref[...], pad_ref)
        scaled = values * to_channels(scale_ref[...], group, per_group, channels)
        value_ref[...] = scaled.astype(jnp.bfloat16)
        out_w_ref[...] = convolve(
            halo_w_ref, write_ref, of_group(taps_w_ref, group), pad_w_ref
        ).astype(jnp.bfloat16)
        carried = jnp.zeros((state, channels), jnp.float32)
        place = lax.broadcasted_iota(jnp.int32, (heads, 8), 1)
        lasts = sum_ref[:, length - 1 :]
        for b in range(blocks):
            lasts = jnp.where(place == b, cum_ref[:, (b + 1) * span - 1 : (b + 1) * span], lasts)
        ends = to_channels(jnp.exp(lasts), group, per_group, channels)
        for b in range(blocks):
            enter_ref[b * state : (b + 1) * state] = carried.astype(jnp.bfloat16)
            here = lax.dot_general(
                out_w_ref[b * span : (b + 1) * span], value_ref[b * span : (b + 1) * span],
                (((0,), (0,)), ((), ())), preferred_element_type=jnp.float32,
            )
            carried = ends[b : b + 1] * (carried + here)
        close_ref[:state] = carried.astype(jnp.bfloat16)
        close_ref[state:] = jnp.broadcast_to(ends[7:8], (16, channels)).astype(jnp.bfloat16)

    by_group = lambda rows, width: pl.BlockSpec((rows, width), lambda g: (0, g))
    whole = lambda rows, width: pl.BlockSpec((rows, width), lambda g: (0, 0))
    return pl.pallas_call(
        kernel,
        grid=(groups,),
        in_specs=[
            by_group(length, channels), by_group(length, state),
            by_group(lead, channels), pl.BlockSpec((lead, state), lambda g: (0, skip + g)),
            by_group(taps.shape[0], channels), pl.BlockSpec(write_taps.shape, lambda g: (0, 0, 0)),
            whole(heads, length), whole(1, heads), whole(1, heads),
        ],
        out_specs=[
            by_group(length, channels), by_group(length, state), whole(heads, length),
            whole(heads, length), by_group(blocks * state, channels), by_group(state + 16, channels),
        ],
        out_shape=[
            jax.ShapeDtypeStruct((length, groups * channels), jnp.bfloat16),
            jax.ShapeDtypeStruct((length, groups * state), jnp.bfloat16),
            jax.ShapeDtypeStruct((heads, length), jnp.float32),
            jax.ShapeDtypeStruct((heads, length), jnp.float32),
            jax.ShapeDtypeStruct((blocks * state, groups * channels), jnp.bfloat16),
            jax.ShapeDtypeStruct((state + 16, groups * channels), jnp.bfloat16),
        ],
        scratch_shapes=[
            pltpu.VMEM((heads, length), jnp.float32),
            pltpu.VMEM((lead + length, channels), jnp.float32),
            pltpu.VMEM((lead + length, state), jnp.float32),
        ],
        compiler_params=pltpu.CompilerParams(dimension_semantics=("arbitrary",), vmem_limit_bytes=MIXER_LIMIT),
        name="mixer_states",
    )(act, writes, halo, halo, taps, write_taps, raw, bias, decay)


def mixer_local(reads, halo, read_taps, values, writes, entering, cum, groups, span):
    heads, length = cum.shape
    channels, state = values.shape[1] // groups, read_taps.shape[2]
    per_group = heads // groups
    blocks = length // span
    lead = halo.shape[0]
    skip = values.shape[1] // state + groups

    def kernel(read_ref, halo_ref, taps_ref, value_ref, write_ref, enter_ref, cum_ref, out_ref,
               out_r_ref, pad_ref):
        group = pl.program_id(0)
        out_r_ref[...] = convolve(
            halo_ref, read_ref, of_group(taps_ref, group), pad_ref
        ).astype(jnp.bfloat16)
        grown = to_channels(jnp.exp(cum_ref[...]), group, per_group, channels)
        row = lax.broadcasted_iota(jnp.int32, (span, span), 0)
        column = lax.broadcasted_iota(jnp.int32, (span, span), 1)
        for b in range(blocks):
            at = slice(b * span, (b + 1) * span)
            meet = lax.dot_general(
                out_r_ref[at], write_ref[at], (((1,), (1,)), ((), ())),
                preferred_element_type=jnp.float32,
            )
            meet = jnp.where(row >= column, meet, 0.0).astype(jnp.bfloat16)
            total = dot32(meet, value_ref[at])
            if b:
                total += dot32(out_r_ref[at], enter_ref[b * state : (b + 1) * state])
            out_ref[at] = grown[at] * total

    by_group = lambda rows, width: pl.BlockSpec((rows, width), lambda g: (0, g))
    return pl.pallas_call(
        kernel,
        grid=(groups,),
        in_specs=[
            pl.BlockSpec((length, state), lambda g: (0, groups + g)),
            pl.BlockSpec((lead, state), lambda g: (0, skip + g)), pl.BlockSpec(read_taps.shape, lambda g: (0, 0, 0)), by_group(length, channels),
            by_group(length, state), by_group(blocks * state, channels),
            pl.BlockSpec((heads, length), lambda g: (0, 0)),
        ],
        out_specs=[by_group(length, channels), by_group(length, state)],
        out_shape=[
            jax.ShapeDtypeStruct((length, groups * channels), jnp.float32),
            jax.ShapeDtypeStruct((length, groups * state), jnp.bfloat16),
        ],
        scratch_shapes=[pltpu.VMEM((lead + length, state), jnp.float32)],
        compiler_params=pltpu.CompilerParams(dimension_semantics=("arbitrary",), vmem_limit_bytes=MIXER_LIMIT),
        cost_estimate=pl.CostEstimate(
            flops=4 * 10**9, bytes_accessed=4 * 10**6, transcendentals=length * groups * state
        ),
        name="mixer_local",
    )(reads, halo, read_taps, values, writes, entering, cum)


def mixer_mix(local, reads, sums, arriving, gates, gain, groups):
    heads, length = sums.shape
    channels, state = local.shape[1] // groups, reads.shape[1] // groups
    per_group = heads // groups

    def kernel(local_ref, read_ref, sum_ref, arrive_ref, gate_ref, gain_ref, out_ref):
        group = pl.program_id(0)
        grown = to_channels(jnp.exp(sum_ref[...]), group, per_group, channels)
        y = local_ref[...] + grown * dot32(read_ref[...], arrive_ref[...])
        gated = y * silu(gate_ref[...].astype(jnp.float32))
        row = lax.broadcasted_iota(jnp.int32, (channels, channels), 0) // (channels // per_group)
        column = lax.broadcasted_iota(jnp.int32, (channels, channels), 1) // (channels // per_group)
        same = jnp.where(row == column, per_group / channels, 0.0).astype(jnp.bfloat16)
        mean = dot32((gated * gated).astype(jnp.bfloat16), same)
        out_ref[...] = (gated * lax.rsqrt(mean + EPS) * gain_ref[...]).astype(jnp.bfloat16)

    by_group = lambda rows, width: pl.BlockSpec((rows, width), lambda g: (0, g))
    return pl.pallas_call(
        kernel,
        grid=(groups,),
        in_specs=[
            by_group(length, channels), by_group(length, state),
            pl.BlockSpec((heads, length), lambda g: (0, 0)),
            by_group(state, channels), by_group(length, channels), by_group(1, channels),
        ],
        out_specs=by_group(length, channels),
        out_shape=jax.ShapeDtypeStruct((length, groups * channels), jnp.bfloat16),
        compiler_params=pltpu.CompilerParams(dimension_semantics=("arbitrary",), vmem_limit_bytes=VMEM_LIMIT),
        name="mixer_mix",
    )(local, reads, sums, arriving, gates, gain)


def project_share(mixed, weight, own, mask, shares):
    length, full = mixed.shape
    width = weight.shape[1] // shares

    def kernel(own_ref, mixed_ref, weight_ref, out_ref):
        out_ref[...] = dot32(mixed_ref[...], weight_ref[...]).astype(jnp.bfloat16)

    return pl.pallas_call(
        kernel,
        grid_spec=pltpu.PrefetchScalarGridSpec(
            num_scalar_prefetch=1,
            grid=(1,),
            in_specs=[
                pl.BlockSpec((length, full), lambda i, o: (0, 0)),
                pl.BlockSpec((full, width), lambda i, o: (0, o[0] ^ mask)),
            ],
            out_specs=pl.BlockSpec((length, width), lambda i, o: (0, 0)),
        ),
        out_shape=jax.ShapeDtypeStruct((length, width), jnp.bfloat16),
        compiler_params=pltpu.CompilerParams(vmem_limit_bytes=VMEM_LIMIT),
        name="project_share",
    )(own, mixed, weight)


def sent_states(closing, state):
    core = lax.axis_index("sp") % 2
    count = lax.axis_size("sp")
    half = closing.shape[1] // 2
    other = swap_core(closing)
    part = lambda rows: lax.dynamic_slice_in_dim(rows, core * half, half, 1).astype(jnp.float32)
    mine, theirs = part(closing), part(other)
    early = jnp.where(core == 0, mine, theirs)
    late = jnp.where(core == 0, theirs, mine)
    decay = late[state : state + 1]
    chip = jnp.concatenate([early[:state] * decay + late[:state], early[state:] * decay], axis=0)
    chip = chip.astype(jnp.bfloat16)
    sent = []
    for k in range(1, count // 2):
        pairs = [(i, i + 2 * k) for i in range(count - 2 * k)]
        sent.append(lax.ppermute(chip, "sp", pairs))
    return sent, other


def arriving_state(sent, other, state):
    core = lax.axis_index("sp") % 2
    total = jnp.zeros((state, sent[0].shape[1]), jnp.float32)
    for rows in reversed(sent):
        rows = rows.astype(jnp.float32)
        total = rows[:state] + rows[state : state + 1] * total
    total = total.astype(jnp.bfloat16)
    swapped = swap_core(total)
    low = jnp.where(core == 0, total, swapped)
    high = jnp.where(core == 0, swapped, total)
    both = jnp.concatenate([low, high], axis=1)
    before = other.astype(jnp.float32)
    after = before[:state] + before[state : state + 1] * both.astype(jnp.float32)
    return jnp.where(core == 0, both, after.astype(jnp.bfloat16))


def per_device(
    stream,
    inner_act,
    gate_act,
    state_write,
    state_read,
    step_raw,
    conv_inner,
    conv_write,
    conv_read,
    step_bias,
    decay_log,
    inner_gain,
    out_weight,
    ffn_gain,
    expert_ids,
    expert_weights,
    expert_gate,
    expert_up,
    expert_down,
):
    length = inner_act.shape[0]
    groups_here = state_write.shape[1]
    state_dim = state_write.shape[2]
    write_width = groups_here * state_dim
    tail_rows = [inner_act[length - LEAD :]]
    tail_rows += [a[length - LEAD :].reshape(LEAD, write_width) for a in (state_write, state_read)]
    halo = from_behind(jnp.concatenate(tail_rows, axis=1), "sp", 1)
    joined = jnp.concatenate(
        [a.reshape(length, write_width) for a in (state_write, state_read)], axis=1
    )
    own_tp = lax.axis_index("tp")
    own_sp = lax.axis_index("sp")
    own_index = own_tp.astype(jnp.int32).reshape(1)
    tp_count = lax.axis_size("tp")
    chips = lax.axis_size("sp") // 2
    values, writes, cum, sums, entering, closing = mixer_states(
        inner_act,
        joined,
        halo,
        conv_inner,
        conv_write,
        step_raw.T,
        step_bias[None],
        decay_log[None],
        groups_here,
        SPAN,
    )
    sent, other = sent_states(closing, state_dim)
    local, reads = mixer_local(
        joined,
        halo,
        conv_read,
        values,
        writes,
        entering,
        cum,
        groups_here,
        SPAN,
    )
    local_experts = expert_gate.shape[0]
    ids_own = expert_ids.T
    ids_other = swap_core(ids_own)
    ids_of = [jnp.concatenate([ids_own, ids_other], axis=0)]
    for k in range(1, chips):
        ids_of.append(move_chips(ids_of[0], k))
    arrive_ranks, leave_ranks, shares = routing_tables(
        jnp.concatenate(ids_of, axis=0),
        expert_weights.T,
        own_sp.astype(jnp.int32).reshape(1),
        local_experts,
    )
    out_width = expert_down.shape[2]
    own_start = own_tp * out_width
    share_of = lax.dynamic_slice_in_dim(stream, own_start, out_width, 1)
    gain_share = lax.dynamic_slice_in_dim(ffn_gain, own_start, out_width, 0)
    inverse = jnp.broadcast_to((1.0 / (ffn_gain * ffn_gain))[:, None], (ffn_gain.shape[0], 128))
    inverse = inverse.astype(jnp.bfloat16)
    arriving = arriving_state(sent, other, state_dim)
    mixed = mixer_mix(local, reads, sums, arriving, gate_act, inner_gain[None], groups_here)
    partials = []
    for m in reversed(range(tp_count)):
        share = project_share(mixed, out_weight, own_index, m, tp_count)
        if m:
            share = swap_tp(share, m)
        partials.append(share.astype(jnp.float32))
    projected = partials[-1]
    for part in partials[:-1]:
        projected = projected + part
    kept = share_of.astype(jnp.float32) + projected
    rows = (kept * gain_share[None, :]).astype(jnp.bfloat16)
    blocks_of = []
    for k in range(chips):
        if k:
            rows = move_chips(rows, 1)
        blocks_of.append([rows, swap_core(rows)])
    chunks = [[k] for k in range(chips)]
    returned = []
    for i, chunk in enumerate(chunks):
        mask, hidden_mask = RELAYS[i % 4]
        picked = pick_rows(
            [rows for k in chunk for rows in blocks_of[k]],
            arrive_ranks,
            [2 * k + side for k in chunk for side in range(2)],
        ).reshape(-1, out_width)
        pieces = gather_tp(picked, mask)
        hidden = hidden_units(pieces, expert_gate, expert_up, inverse, own_index)
        pieces = gather_tp(hidden, hidden_mask)
        given = expert_rows(pieces, expert_down, own_index)
        for j, k in enumerate(chunk):
            for side in range(2):
                home = given[2 * j + side]
                if k or side:
                    home = move_chips(home, -k, bool(side))
                returned.append((2 * k + side, home))
    returned = returned[2:-2] + returned[-2:] + returned[:2]
    late = 4
    total = kept
    for part, kind in ((returned[:-late], jnp.float32), (returned[-late:], jnp.bfloat16)):
        places, rows = zip(*part)
        total = combine(total, rows, places, leave_ranks, shares, kind)
    return total


RELAYS = ((2, 1), (1, 2), (2, 2), (1, 2))


def solution(mesh):
    return jax.shard_map(
        per_device,
        mesh=mesh,
        in_specs=(
            P("sp", None),
            P("sp", "tp"),
            P("sp", "tp"),
            P("sp", "tp", None),
            P("sp", "tp", None),
            P("sp", "tp"),
            P(None, "tp"),
            P(None, "tp", None),
            P(None, "tp", None),
            P("tp"),
            P("tp"),
            P("tp"),
            P("tp", None),
            P(),
            P("sp", None),
            P("sp", None),
            P("sp", None, "tp"),
            P("sp", None, "tp"),
            P("sp", None, "tp"),
        ),
        out_specs=P("sp", "tp"),
        check_vma=False,
    )
```

```python
import jax
import jax.numpy as jnp
from jax import lax
from jax.experimental import pallas as pl
from jax.experimental.pallas import tpu as pltpu
from jax.sharding import PartitionSpec as P

SPAN = 128
LEAD = 16
VMEM_LIMIT = 16 * 2**20
MIXER_LIMIT = 60 * 2**20
TOPK = 2
CAP = 48


EPS = 1e-06


def from_behind(value, axis, steps):
    count = lax.axis_size(axis)
    first, last = (max(0, -steps), min(count, count - steps))
    return lax.ppermute(value, axis, [(source, source + steps) for source in range(first, last)])


def silu(x):
    return x * (0.5 * jnp.tanh(0.5 * x) + 0.5)


def swap_core(value):
    count = lax.axis_size("sp")
    return lax.ppermute(value, "sp", [(i, i ^ 1) for i in range(count)])


def move_chips(value, steps, cross=False):
    count = lax.axis_size("sp")
    return lax.ppermute(
        value, "sp", [(i, ((i + 2 * steps) % count) ^ int(cross)) for i in range(count)]
    )


def swap_tp(value, mask):
    count = lax.axis_size("tp")
    return lax.ppermute(value, "tp", [(i, i ^ mask) for i in range(count)])


def gather_tp(rows, mask):
    count = lax.axis_size("tp")
    if count != 4:
        every = lax.all_gather(rows, "tp")
        own = lax.axis_index("tp")
        return [lax.dynamic_index_in_dim(every, own ^ m, 0, False) for m in range(count)]
    near = swap_tp(rows, mask)
    other = swap_tp(rows, 3 - mask)
    far = swap_tp(near, 3 - mask)
    return [rows, near, other, far] if mask == 1 else [rows, other, near, far]


def routing_tables(ids, weights, own, experts):
    blocks = ids.shape[0] // TOPK
    tokens = ids.shape[1]
    shape = (blocks, experts, tokens)

    def kernel(own_ref, ids_ref, weight_ref, arrive_ref, leave_ref, share_ref):
        expert = lax.broadcasted_iota(jnp.int32, (experts, tokens), 0)
        first = own_ref[0] * experts
        named = []
        for b in range(blocks):
            rows = [ids_ref[TOPK * b + j : TOPK * b + j + 1] for j in range(TOPK)]
            named.append(sum((row == expert + first).astype(jnp.float32) for row in rows))
        own_rows = [ids_ref[j : j + 1] for j in range(TOPK)]
        for b in range(blocks):
            owner = ((own_ref[0] + 2 * (b // 2)) % blocks) ^ (b % 2)
            hits = [(row == expert + owner * experts).astype(jnp.float32) for row in own_rows]
            named.append(sum(hits))
            share_ref[b] = sum(hit * weight_ref[j : j + 1] for j, hit in enumerate(hits))
        every = jnp.concatenate(named, axis=0)
        row = lax.broadcasted_iota(jnp.int32, (tokens, tokens), 0)
        column = lax.broadcasted_iota(jnp.int32, (tokens, tokens), 1)
        slots = dot32(every.astype(jnp.bfloat16), (row < column).astype(jnp.bfloat16))
        slots = jnp.where(every > 0, slots.astype(jnp.int32), -1)
        for b in range(blocks):
            arrive_ref[b] = slots[b * experts : (b + 1) * experts]
            leave_ref[b] = slots[(blocks + b) * experts : (blocks + b + 1) * experts]

    return pl.pallas_call(
        kernel,
        in_specs=[
            pl.BlockSpec(memory_space=pltpu.SMEM), pl.BlockSpec(memory_space=pltpu.VMEM),
            pl.BlockSpec(memory_space=pltpu.VMEM),
        ],
        out_shape=[
            jax.ShapeDtypeStruct(shape, jnp.int32), jax.ShapeDtypeStruct(shape, jnp.int32),
            jax.ShapeDtypeStruct(shape, jnp.float32),
        ],
        compiler_params=pltpu.CompilerParams(vmem_limit_bytes=VMEM_LIMIT),
        name="routing_tables",
    )(own, ids, weights)


def pick_rows(blocks, ranks, places):
    experts = ranks.shape[1]
    tokens, width = blocks[0].shape
    count = len(blocks)

    def kernel(*refs):
        block_refs, rank_ref, out_ref = refs[:count], refs[count], refs[-1]
        slot = lax.broadcasted_iota(jnp.int32, (CAP, tokens), 0)
        for side, rows in enumerate(block_refs):
            rank = rank_ref[places[side]]
            chosen = jnp.concatenate(
                [(rank[e : e + 1, :] == slot).astype(jnp.float32) for e in range(experts)], axis=0
            ).astype(jnp.bfloat16)
            picked = dot32(chosen, rows[...]).astype(jnp.bfloat16)
            for e in range(experts):
                out_ref[e, side] = picked[e * CAP : (e + 1) * CAP]

    return pl.pallas_call(
        kernel,
        out_shape=jax.ShapeDtypeStruct((experts, count, CAP, width), jnp.bfloat16),
        cost_estimate=pl.CostEstimate(
            flops=2 * count * experts * CAP * tokens * width,
            bytes_accessed=4 * count * tokens * width,
            transcendentals=0,
        ),
        compiler_params=pltpu.CompilerParams(vmem_limit_bytes=VMEM_LIMIT),
        name="pick_rows",
    )(*blocks, ranks)


def hidden_units(pieces, gate, up, inverse, own):
    experts, full, units = gate.shape
    rows, width = pieces[0].shape
    each = rows // experts
    count = len(pieces)
    lanes = inverse.shape[1]

    def kernel(own_ref, *refs):
        parts, (gate_ref, up_ref, inverse_ref, out_ref) = refs[:count], refs[count:]
        gate_sum = jnp.zeros((each, units), jnp.float32)
        up_sum = jnp.zeros((each, units), jnp.float32)
        squares = jnp.zeros((each, lanes), jnp.float32)
        for m in range(count):
            part = parts[m][...]
            at = pl.ds(pl.multiple_of((own_ref[0] ^ m) * width, width), width)
            gate_sum += dot32(part, gate_ref[0, at, :])
            up_sum += dot32(part, up_ref[0, at, :])
            squares += dot32(part * part, inverse_ref[at, :])
        scale = lax.rsqrt(squares[:, :1] / full + EPS)
        out_ref[...] = (silu(gate_sum * scale) * (up_sum * scale)).astype(jnp.bfloat16)

    return pl.pallas_call(
        kernel,
        grid_spec=pltpu.PrefetchScalarGridSpec(
            num_scalar_prefetch=1,
            grid=(experts,),
            in_specs=[pl.BlockSpec((each, width), lambda e, o: (e, 0)) for _ in range(count)]
            + [pl.BlockSpec((1, full, units), lambda e, o: (e, 0, 0)) for _ in range(2)]
            + [pl.BlockSpec((full, lanes), lambda e, o: (0, 0))],
            out_specs=pl.BlockSpec((each, units), lambda e, o: (e, 0)),
        ),
        out_shape=jax.ShapeDtypeStruct((rows, units), jnp.bfloat16),
        cost_estimate=pl.CostEstimate(
            flops=4 * rows * full * units,
            bytes_accessed=4 * experts * full * units,
            transcendentals=rows * units,
        ),
        compiler_params=pltpu.CompilerParams(vmem_limit_bytes=VMEM_LIMIT),
        name="hidden_units",
    )(own, *pieces, gate, up, inverse)


def expert_rows(pieces, down, own):
    experts, full, columns = down.shape
    rows, units = pieces[0].shape
    each = rows // experts
    blocks = each // CAP
    count = len(pieces)

    def kernel(own_ref, *refs):
        parts, down_ref, outs = refs[:count], refs[count], refs[count + 1 :]
        total = jnp.zeros((each, columns), jnp.float32)
        for m in range(count):
            at = pl.ds(pl.multiple_of((own_ref[0] ^ m) * units, units), units)
            total += dot32(parts[m][...], down_ref[0, at, :])
        for i in range(blocks):
            outs[i][...] = total[i * CAP : (i + 1) * CAP].astype(jnp.bfloat16)

    return pl.pallas_call(
        kernel,
        grid_spec=pltpu.PrefetchScalarGridSpec(
            num_scalar_prefetch=1,
            grid=(experts,),
            in_specs=[pl.BlockSpec((each, units), lambda e, o: (e, 0)) for _ in range(count)]
            + [pl.BlockSpec((1, full, columns), lambda e, o: (e, 0, 0))],
            out_specs=[pl.BlockSpec((CAP, columns), lambda e, o: (e, 0)) for _ in range(blocks)],
        ),
        out_shape=[jax.ShapeDtypeStruct((experts * CAP, columns), jnp.bfloat16) for _ in range(blocks)],
        cost_estimate=pl.CostEstimate(
            flops=2 * rows * full * columns,
            bytes_accessed=2 * experts * full * columns,
            transcendentals=0,
        ),
        compiler_params=pltpu.CompilerParams(vmem_limit_bytes=VMEM_LIMIT),
        name="expert_rows",
    )(own, *pieces, down)


def combine(total, returned, places, ranks, shares, kind):
    tokens, columns = total.shape
    count = len(returned)
    experts = ranks.shape[1]

    def kernel(total_ref, *refs):
        rows_refs, rank_ref, share_ref, out_ref = refs[:count], refs[-3], refs[-2], refs[-1]
        slot = lax.broadcasted_iota(jnp.int32, (CAP, tokens), 0)
        value = total_ref[...]
        for place, rows in zip(places, rows_refs):
            rank, share = rank_ref[place], share_ref[place]
            chosen = jnp.concatenate(
                [
                    jnp.where(rank[e : e + 1, :] == slot, share[e : e + 1, :], 0.0)
                    for e in range(experts)
                ],
                axis=0,
            )
            for part in halves(chosen):
                value += lax.dot_general(
                    part, rows[...], (((0,), (0,)), ((), ())), preferred_element_type=jnp.float32
                )
        out_ref[...] = value.astype(kind)

    return pl.pallas_call(
        kernel,
        out_shape=jax.ShapeDtypeStruct((tokens, columns), kind),
        cost_estimate=pl.CostEstimate(
            flops=4 * count * tokens * experts * CAP * columns,
            bytes_accessed=8 * tokens * columns,
            transcendentals=0,
        ),
        compiler_params=pltpu.CompilerParams(vmem_limit_bytes=VMEM_LIMIT),
        name="combine",
    )(total, *returned, ranks, shares)


def halves(value):
    high = value.astype(jnp.bfloat16)
    return high, (value - high.astype(jnp.float32)).astype(jnp.bfloat16)


def column(row):
    size = row.shape[1]
    same = lax.broadcasted_iota(jnp.int32, (size, size), 0) == lax.broadcasted_iota(
        jnp.int32, (size, size), 1
    )
    return jnp.sum(jnp.where(same, row, 0.0), axis=1, keepdims=True)


def dot32(left, right):
    return jnp.dot(left, right, preferred_element_type=jnp.float32)


def to_channels(value, group, per_group, channels):
    heads = value.shape[0]
    row = lax.broadcasted_iota(jnp.int32, (heads, channels), 0)
    column = lax.broadcasted_iota(jnp.int32, (heads, channels), 1)
    spread = (row == group * per_group + column // (channels // per_group)).astype(jnp.bfloat16)
    high, low = halves(value)
    over = (((0,), (0,)), ((), ()))
    return lax.dot_general(
        high, spread, over, preferred_element_type=jnp.float32
    ) + lax.dot_general(low, spread, over, preferred_element_type=jnp.float32)


def of_group(taps, group):
    place = lax.broadcasted_iota(jnp.int32, taps.shape, 1)
    return jnp.sum(jnp.where(place == group, taps[...].astype(jnp.float32), 0.0), axis=1)


def convolve(halo, rows, taps, scratch):
    lead, length = halo.shape[0], rows.shape[0]
    weights = taps.astype(jnp.float32)
    count = weights.shape[0]
    scratch[:lead] = halo[...].astype(jnp.float32)
    scratch[lead:] = rows[...].astype(jnp.float32)
    total = weights[0:1] * scratch[lead - count + 1 : lead - count + 1 + length]
    for k in range(1, count):
        total += weights[k : k + 1] * scratch[lead - count + 1 + k : lead - count + 1 + k + length]
    return silu(total)


def mixer_states(act, writes, halo, taps, write_taps, raw, bias, decay, groups, span):
    heads, length = raw.shape
    channels, state = act.shape[1] // groups, write_taps.shape[2]
    per_group = heads // groups
    blocks = length // span
    lead = halo.shape[0]
    skip = act.shape[1] // state

    def kernel(act_ref, write_ref, halo_ref, halo_w_ref, taps_ref, taps_w_ref, raw_ref, bias_ref,
               decay_ref, value_ref, out_w_ref, cum_ref, sum_ref, enter_ref, close_ref, scale_ref,
               pad_ref, pad_w_ref):
        group = pl.program_id(0)

        @pl.when(group == 0)
        def _():
            x = raw_ref[...].astype(jnp.float32) + column(bias_ref[...])
            step = jnp.maximum(x, 0.0) + jnp.log1p(jnp.exp(-jnp.abs(x)))
            logs = step * -jnp.exp(column(decay_ref[...]))
            row = lax.broadcasted_iota(jnp.int32, (span, span), 0)
            upto = (row <= lax.broadcasted_iota(jnp.int32, (span, span), 1)).astype(jnp.bfloat16)
            base = jnp.zeros((heads, 1), jnp.float32)
            for b in range(blocks):
                at = slice(b * span, (b + 1) * span)
                part = logs[:, at]
                high, low = halves(part)
                rest = (part - high.astype(jnp.float32) - low.astype(jnp.float32)).astype(jnp.bfloat16)
                cum = dot32(high, upto) + dot32(low, upto) + dot32(rest, upto)
                cum_ref[:, at] = cum
                sum_ref[:, at] = cum + base
                scale_ref[:, at] = step[:, at] * jnp.exp(-cum)
                base = base + cum[:, span - 1 : span]

        values = convolve(halo_ref, act_ref, taps_ref[...], pad_ref)
        scaled = values * to_channels(scale_ref[...], group, per_group, channels)
        value_ref[...] = scaled.astype(jnp.bfloat16)
        out_w_ref[...] = convolve(
            halo_w_ref, write_ref, of_group(taps_w_ref, group), pad_w_ref
        ).astype(jnp.bfloat16)
        carried = jnp.zeros((state, channels), jnp.float32)
        place = lax.broadcasted_iota(jnp.int32, (heads, 8), 1)
        lasts = sum_ref[:, length - 1 :]
        for b in range(blocks):
            lasts = jnp.where(place == b, cum_ref[:, (b + 1) * span - 1 : (b + 1) * span], lasts)
        ends = to_channels(jnp.exp(lasts), group, per_group, channels)
        for b in range(blocks):
            enter_ref[b * state : (b + 1) * state] = carried.astype(jnp.bfloat16)
            here = lax.dot_general(
                out_w_ref[b * span : (b + 1) * span], value_ref[b * span : (b + 1) * span],
                (((0,), (0,)), ((), ())), preferred_element_type=jnp.float32,
            )
            carried = ends[b : b + 1] * (carried + here)
        close_ref[:state] = carried.astype(jnp.bfloat16)
        close_ref[state:] = jnp.broadcast_to(ends[7:8], (16, channels)).astype(jnp.bfloat16)

    by_group = lambda rows, width: pl.BlockSpec((rows, width), lambda g: (0, g))
    whole = lambda rows, width: pl.BlockSpec((rows, width), lambda g: (0, 0))
    return pl.pallas_call(
        kernel,
        grid=(groups,),
        in_specs=[
            by_group(length, channels), by_group(length, state),
            by_group(lead, channels), pl.BlockSpec((lead, state), lambda g: (0, skip + g)),
            by_group(taps.shape[0], channels), pl.BlockSpec(write_taps.shape, lambda g: (0, 0, 0)),
            whole(heads, length), whole(1, heads), whole(1, heads),
        ],
        out_specs=[
            by_group(length, channels), by_group(length, state), whole(heads, length),
            whole(heads, length), by_group(blocks * state, channels), by_group(state + 16, channels),
        ],
        out_shape=[
            jax.ShapeDtypeStruct((length, groups * channels), jnp.bfloat16),
            jax.ShapeDtypeStruct((length, groups * state), jnp.bfloat16),
            jax.ShapeDtypeStruct((heads, length), jnp.float32),
            jax.ShapeDtypeStruct((heads, length), jnp.float32),
            jax.ShapeDtypeStruct((blocks * state, groups * channels), jnp.bfloat16),
            jax.ShapeDtypeStruct((state + 16, groups * channels), jnp.bfloat16),
        ],
        scratch_shapes=[
            pltpu.VMEM((heads, length), jnp.float32),
            pltpu.VMEM((lead + length, channels), jnp.float32),
            pltpu.VMEM((lead + length, state), jnp.float32),
        ],
        compiler_params=pltpu.CompilerParams(dimension_semantics=("arbitrary",), vmem_limit_bytes=MIXER_LIMIT),
        name="mixer_states",
    )(act, writes, halo, halo, taps, write_taps, raw, bias, decay)


def mixer_local(reads, halo, read_taps, values, writes, entering, cum, groups, span):
    heads, length = cum.shape
    channels, state = values.shape[1] // groups, read_taps.shape[2]
    per_group = heads // groups
    blocks = length // span
    lead = halo.shape[0]
    skip = values.shape[1] // state + groups

    def kernel(read_ref, halo_ref, taps_ref, value_ref, write_ref, enter_ref, cum_ref, out_ref,
               out_r_ref, pad_ref):
        group = pl.program_id(0)
        out_r_ref[...] = convolve(
            halo_ref, read_ref, of_group(taps_ref, group), pad_ref
        ).astype(jnp.bfloat16)
        grown = to_channels(jnp.exp(cum_ref[...]), group, per_group, channels)
        row = lax.broadcasted_iota(jnp.int32, (span, span), 0)
        column = lax.broadcasted_iota(jnp.int32, (span, span), 1)
        for b in range(blocks):
            at = slice(b * span, (b + 1) * span)
            meet = lax.dot_general(
                out_r_ref[at], write_ref[at], (((1,), (1,)), ((), ())),
                preferred_element_type=jnp.float32,
            )
            meet = jnp.where(row >= column, meet, 0.0).astype(jnp.bfloat16)
            total = dot32(meet, value_ref[at])
            if b:
                total += dot32(out_r_ref[at], enter_ref[b * state : (b + 1) * state])
            out_ref[at] = grown[at] * total

    by_group = lambda rows, width: pl.BlockSpec((rows, width), lambda g: (0, g))
    return pl.pallas_call(
        kernel,
        grid=(groups,),
        in_specs=[
            pl.BlockSpec((length, state), lambda g: (0, groups + g)),
            pl.BlockSpec((lead, state), lambda g: (0, skip + g)), pl.BlockSpec(read_taps.shape, lambda g: (0, 0, 0)), by_group(length, channels),
            by_group(length, state), by_group(blocks * state, channels),
            pl.BlockSpec((heads, length), lambda g: (0, 0)),
        ],
        out_specs=[by_group(length, channels), by_group(length, state)],
        out_shape=[
            jax.ShapeDtypeStruct((length, groups * channels), jnp.float32),
            jax.ShapeDtypeStruct((length, groups * state), jnp.bfloat16),
        ],
        scratch_shapes=[pltpu.VMEM((lead + length, state), jnp.float32)],
        compiler_params=pltpu.CompilerParams(dimension_semantics=("arbitrary",), vmem_limit_bytes=MIXER_LIMIT),
        cost_estimate=pl.CostEstimate(
            flops=4 * 10**9, bytes_accessed=4 * 10**6, transcendentals=length * groups * state
        ),
        name="mixer_local",
    )(reads, halo, read_taps, values, writes, entering, cum)


def mixer_mix(local, reads, sums, arriving, gates, gain, groups):
    heads, length = sums.shape
    channels, state = local.shape[1] // groups, reads.shape[1] // groups
    per_group = heads // groups

    def kernel(local_ref, read_ref, sum_ref, arrive_ref, gate_ref, gain_ref, out_ref):
        group = pl.program_id(0)
        grown = to_channels(jnp.exp(sum_ref[...]), group, per_group, channels)
        y = local_ref[...] + grown * dot32(read_ref[...], arrive_ref[...])
        gated = y * silu(gate_ref[...].astype(jnp.float32))
        row = lax.broadcasted_iota(jnp.int32, (channels, channels), 0) // (channels // per_group)
        column = lax.broadcasted_iota(jnp.int32, (channels, channels), 1) // (channels // per_group)
        same = jnp.where(row == column, per_group / channels, 0.0).astype(jnp.bfloat16)
        mean = dot32((gated * gated).astype(jnp.bfloat16), same)
        out_ref[...] = (gated * lax.rsqrt(mean + EPS) * gain_ref[...]).astype(jnp.bfloat16)

    by_group = lambda rows, width: pl.BlockSpec((rows, width), lambda g: (0, g))
    return pl.pallas_call(
        kernel,
        grid=(groups,),
        in_specs=[
            by_group(length, channels), by_group(length, state),
            pl.BlockSpec((heads, length), lambda g: (0, 0)),
            by_group(state, channels), by_group(length, channels), by_group(1, channels),
        ],
        out_specs=by_group(length, channels),
        out_shape=jax.ShapeDtypeStruct((length, groups * channels), jnp.bfloat16),
        compiler_params=pltpu.CompilerParams(dimension_semantics=("arbitrary",), vmem_limit_bytes=VMEM_LIMIT),
        name="mixer_mix",
    )(local, reads, sums, arriving, gates, gain)


def project_share(mixed, weight, own, mask, shares):
    length, full = mixed.shape
    width = weight.shape[1] // shares

    def kernel(own_ref, mixed_ref, weight_ref, out_ref):
        out_ref[...] = dot32(mixed_ref[...], weight_ref[...]).astype(jnp.bfloat16)

    return pl.pallas_call(
        kernel,
        grid_spec=pltpu.PrefetchScalarGridSpec(
            num_scalar_prefetch=1,
            grid=(1,),
            in_specs=[
                pl.BlockSpec((length, full), lambda i, o: (0, 0)),
                pl.BlockSpec((full, width), lambda i, o: (0, o[0] ^ mask)),
            ],
            out_specs=pl.BlockSpec((length, width), lambda i, o: (0, 0)),
        ),
        out_shape=jax.ShapeDtypeStruct((length, width), jnp.bfloat16),
        compiler_params=pltpu.CompilerParams(vmem_limit_bytes=VMEM_LIMIT),
        name="project_share",
    )(own, mixed, weight)


def sent_states(closing, state):
    core = lax.axis_index("sp") % 2
    count = lax.axis_size("sp")
    half = closing.shape[1] // 2
    other = swap_core(closing)
    part = lambda rows: lax.dynamic_slice_in_dim(rows, core * half, half, 1).astype(jnp.float32)
    mine, theirs = part(closing), part(other)
    early = jnp.where(core == 0, mine, theirs)
    late = jnp.where(core == 0, theirs, mine)
    decay = late[state : state + 1]
    chip = jnp.concatenate([early[:state] * decay + late[:state], early[state:] * decay], axis=0)
    chip = chip.astype(jnp.bfloat16)
    sent = []
    for k in range(1, count // 2):
        pairs = [(i, i + 2 * k) for i in range(count - 2 * k)]
        sent.append(lax.ppermute(chip, "sp", pairs))
    return sent, other


def arriving_state(sent, other, state):
    core = lax.axis_index("sp") % 2
    total = jnp.zeros((state, sent[0].shape[1]), jnp.float32)
    for rows in reversed(sent):
        rows = rows.astype(jnp.float32)
        total = rows[:state] + rows[state : state + 1] * total
    total = total.astype(jnp.bfloat16)
    swapped = swap_core(total)
    low = jnp.where(core == 0, total, swapped)
    high = jnp.where(core == 0, swapped, total)
    both = jnp.concatenate([low, high], axis=1)
    before = other.astype(jnp.float32)
    after = before[:state] + before[state : state + 1] * both.astype(jnp.float32)
    return jnp.where(core == 0, both, after.astype(jnp.bfloat16))


def per_device(
    stream,
    inner_act,
    gate_act,
    state_write,
    state_read,
    step_raw,
    conv_inner,
    conv_write,
    conv_read,
    step_bias,
    decay_log,
    inner_gain,
    out_weight,
    ffn_gain,
    expert_ids,
    expert_weights,
    expert_gate,
    expert_up,
    expert_down,
):
    length = inner_act.shape[0]
    groups_here = state_write.shape[1]
    state_dim = state_write.shape[2]
    write_width = groups_here * state_dim
    tail_rows = [inner_act[length - LEAD :]]
    tail_rows += [a[length - LEAD :].reshape(LEAD, write_width) for a in (state_write, state_read)]
    halo = from_behind(jnp.concatenate(tail_rows, axis=1), "sp", 1)
    joined = jnp.concatenate(
        [a.reshape(length, write_width) for a in (state_write, state_read)], axis=1
    )
    own_tp = lax.axis_index("tp")
    own_sp = lax.axis_index("sp")
    own_index = own_tp.astype(jnp.int32).reshape(1)
    tp_count = lax.axis_size("tp")
    chips = lax.axis_size("sp") // 2
    values, writes, cum, sums, entering, closing = mixer_states(
        inner_act,
        joined,
        halo,
        conv_inner,
        conv_write,
        step_raw.T,
        step_bias[None],
        decay_log[None],
        groups_here,
        SPAN,
    )
    sent, other = sent_states(closing, state_dim)
    local, reads = mixer_local(
        joined,
        halo,
        conv_read,
        values,
        writes,
        entering,
        cum,
        groups_here,
        SPAN,
    )
    local_experts = expert_gate.shape[0]
    ids_own = expert_ids.T
    ids_other = swap_core(ids_own)
    ids_of = [jnp.concatenate([ids_own, ids_other], axis=0)]
    for k in range(1, chips):
        ids_of.append(move_chips(ids_of[0], k))
    arrive_ranks, leave_ranks, shares = routing_tables(
        jnp.concatenate(ids_of, axis=0),
        expert_weights.T,
        own_sp.astype(jnp.int32).reshape(1),
        local_experts,
    )
    out_width = expert_down.shape[2]
    own_start = own_tp * out_width
    share_of = lax.dynamic_slice_in_dim(stream, own_start, out_width, 1)
    gain_share = lax.dynamic_slice_in_dim(ffn_gain, own_start, out_width, 0)
    inverse = jnp.broadcast_to((1.0 / (ffn_gain * ffn_gain))[:, None], (ffn_gain.shape[0], 128))
    inverse = inverse.astype(jnp.bfloat16)
    arriving = arriving_state(sent, other, state_dim)
    mixed = mixer_mix(local, reads, sums, arriving, gate_act, inner_gain[None], groups_here)
    partials = []
    for m in reversed(range(tp_count)):
        share = project_share(mixed, out_weight, own_index, m, tp_count)
        if m:
            share = swap_tp(share, m)
        partials.append(share.astype(jnp.float32))
    projected = partials[-1]
    for part in partials[:-1]:
        projected = projected + part
    kept = share_of.astype(jnp.float32) + projected
    rows = (kept * gain_share[None, :]).astype(jnp.bfloat16)
    blocks_of = []
    for k in range(chips):
        if k:
            rows = move_chips(rows, 1)
        blocks_of.append([rows, swap_core(rows)])
    chunks = [[k] for k in range(chips)]
    returned = []
    for i, chunk in enumerate(chunks):
        mask, hidden_mask = RELAYS[i % 4]
        picked = pick_rows(
            [rows for k in chunk for rows in blocks_of[k]],
            arrive_ranks,
            [2 * k + side for k in chunk for side in range(2)],
        ).reshape(-1, out_width)
        pieces = gather_tp(picked, mask)
        hidden = hidden_units(pieces, expert_gate, expert_up, inverse, own_index)
        pieces = gather_tp(hidden, hidden_mask)
        given = expert_rows(pieces, expert_down, own_index)
        for j, k in enumerate(chunk):
            for side in range(2):
                home = given[2 * j + side]
                if k or side:
                    home = move_chips(home, -k, bool(side))
                returned.append((2 * k + side, home))
    total = kept
    parts = (returned[2:-2], returned[:2], returned[-2:])
    for part, kind in zip(parts, (jnp.float32, jnp.float32, jnp.bfloat16)):
        places, rows = zip(*part)
        total = combine(total, rows, places, leave_ranks, shares, kind)
    return total


RELAYS = ((1, 1), (2, 1), (1, 1), (2, 2))


def solution(mesh):
    return jax.shard_map(
        per_device,
        mesh=mesh,
        in_specs=(
            P("sp", None),
            P("sp", "tp"),
            P("sp", "tp"),
            P("sp", "tp", None),
            P("sp", "tp", None),
            P("sp", "tp"),
            P(None, "tp"),
            P(None, "tp", None),
            P(None, "tp", None),
            P("tp"),
            P("tp"),
            P("tp"),
            P("tp", None),
            P(),
            P("sp", None),
            P("sp", None),
            P("sp", None, "tp"),
            P("sp", None, "tp"),
            P("sp", None, "tp"),
        ),
        out_specs=P("sp", "tp"),
        check_vma=False,
    )
```
